512 devices in a mesh: sp: 64 (over z, y), tp: 8 (over x, core).
Axes of the slice: x: 4, y: 4, z: 16, core: 2. Of those that a mesh axis runs over, the one named last changes fastest.
Arguments:
- queries: bfloat16 [8192, 1024], P('sp', 'tp'), may hold values from -5 to 5
- keys: bfloat16 [8192, 1024], P('sp', 'tp'), may hold values from -5 to 5
- values: bfloat16 [8192, 1024], P('sp', 'tp'), may hold values from -5 to 5
- in_gate: float32 [8, 8192], P('tp', 'sp'), may hold values from -7 to 213
- forget_gate: float32 [8, 8192], P('tp', 'sp'), may hold values from 0 to 17
- stream: bfloat16 [8192, 2048], P('sp', 'tp'), may hold values from -24 to 24
- head_gain: float32 [1024], replicated, may hold values from 0.1 to 1.9
- out_weight: bfloat16 [1024, 2048], P(None, 'tp'), may hold values from -0.1875 to 0.1875
- norm_gain: float32 [2048], replicated, may hold values from 0.1 to 1.9
- gate_weight: bfloat16 [2048, 5632], P('sp', 'tp'), may hold values from -0.125 to 0.125
- up_weight: bfloat16 [2048, 5632], P('sp', 'tp'), may hold values from -0.125 to 0.125
- down_weight: bfloat16 [2048, 5632], P('sp', 'tp'), may hold values from -0.15625 to 0.15625
Outputs:
- layer_out: float32 [8192, 2048], P('sp', 'tp')
The draws below stay inside these ranges and needn't reach their ends.
All inputs are finite; a program needn't handle non-finite values.
Results may differ from the reference program's by a relative error of at most 0.004.
Values may be sent and summed in bfloat16 or wider, within the bound.
A program may use at most 64 MiB of HBM per device.

```python
import math
import jax
import jax.numpy as jnp
from jax import lax

D = 2048
FF = 5632
MEMORY_HEADS = 8
HEAD_DIM = 128
BLOCK = 128
TOK_DEV = 128
SEQUENCE_TOKENS = 8192
MIX = 1024
N_TP = 8


def draw_stream(key, part):
    noise_key, row_key = jax.random.split(key, 2)
    column = jnp.arange(D, dtype=jnp.float32) / D
    column_scale = jnp.exp(math.log(0.3) + math.log(10.0) * column)[None, :]
    base_draw = jnp.clip(jax.random.normal(noise_key, (SEQUENCE_TOKENS, D), jnp.float32), -4.0, 4.0)
    row_scale = jnp.exp(jax.random.uniform(row_key, (SEQUENCE_TOKENS, 1), jnp.float32, math.log(0.5), math.log(2.0)))
    return (base_draw * row_scale * column_scale).astype(jnp.bfloat16)


def draw_in_gate(key, part):
    noise_key = jax.random.fold_in(key, 0)
    return jnp.clip(-1.0 + 1.5 * jax.random.normal(noise_key, (MEMORY_HEADS, SEQUENCE_TOKENS), jnp.float32), -7.0, 5.0)


def draw_forget_gate(key, part):
    permute_random_key, perturb_random_key, decay_random_key, surge_random_key, retain_random_key = jax.random.split(key, 5)
    slow_level = math.log(4.0 * SEQUENCE_TOKENS)
    head_order = jax.random.permutation(permute_random_key, MEMORY_HEADS)
    fast_heads = head_order < MEMORY_HEADS // 2
    jitter = jnp.clip(jax.random.normal(perturb_random_key, (MEMORY_HEADS, SEQUENCE_TOKENS), jnp.float32), -3.0, 3.0)
    head_level = jnp.where(fast_heads, 4.5, slow_level)[:, None]
    block_rate = jax.random.uniform(decay_random_key, (MEMORY_HEADS, SEQUENCE_TOKENS // TOK_DEV), jnp.float32, 0.0, math.log(4.0))
    block_rate = jnp.repeat(block_rate, TOK_DEV, axis=1)
    gate_outputs = head_level - block_rate + jitter
    surge_position = jax.random.randint(surge_random_key, (MEMORY_HEADS, 2), 0, SEQUENCE_TOKENS)
    surge_retain = jax.random.uniform(retain_random_key, (MEMORY_HEADS, 2), jnp.float32, 0.5, 0.8)
    surge_amount = jnp.log(surge_retain / (1.0 - surge_retain))
    token_position = jnp.arange(SEQUENCE_TOKENS, dtype=jnp.int32)[None, :, None]
    surge_applied = token_position == surge_position[:, None, :]
    surge_magnitude = jnp.min(jnp.where(surge_applied, surge_amount[:, None, :], 100.0), axis=2)
    return jnp.where(jnp.any(surge_applied, axis=2), surge_magnitude, gate_outputs)


def level_of(own_key, dims, cuts, low, high):
    loudness = 1.0
    for axis_at, blocks in cuts:
        heights = jax.random.uniform(jax.random.fold_in(jax.random.fold_in(own_key, 6), axis_at), (blocks,), jnp.float32, low / len(cuts), high / len(cuts))
        loudness = loudness * jnp.repeat(jnp.exp(heights), dims[axis_at] // blocks).reshape((-1,) + (1,) * (len(dims) - 1 - axis_at))
    return loudness


def gaussian(own_key, extent, deviation, limit, shards=(), kind=jnp.bfloat16):
    level = level_of(own_key, extent, shards, -0.22, 0.18) if shards else 1.0
    values = jax.random.normal(own_key, extent, jnp.float32) * deviation * level
    return jnp.minimum(jnp.maximum(values, -limit), limit).astype(kind)


def setup_inputs(seed: int = 0) -> dict:
    key_list = jax.random.split(jax.random.key(seed), 13)
    return {
        "queries": gaussian(key_list[0], (SEQUENCE_TOKENS, MIX), 1.0, 5.0, ((0, 64), (1, 8))),
        "keys": gaussian(key_list[1], (SEQUENCE_TOKENS, MIX), 1.0, 5.0, ((0, 64), (1, 8))),
        "values": gaussian(key_list[2], (SEQUENCE_TOKENS, MIX), 1.0, 5.0, ((0, 64), (1, 8))),
        "in_gate": draw_in_gate(jax.random.fold_in(key_list[12], 71), 0),
        "forget_gate": draw_forget_gate(jax.random.fold_in(key_list[12], 71), 0),
        "stream": draw_stream(jax.random.fold_in(key_list[12], 71), 0),
        "head_gain": jnp.clip(1.0 + 0.18 * jax.random.normal(key_list[6], (MIX,), jnp.float32), 0.1, 1.9),
        "out_weight": gaussian(key_list[7], (MIX, D), MIX ** -0.5, 0.1875, ((1, 8),)),
        "norm_gain": jnp.clip(1.0 + 0.18 * jax.random.normal(key_list[8], (D,), jnp.float32), 0.1, 1.9),
        "gate_weight": gaussian(key_list[9], (D, FF), D ** -0.5, 0.125, ((0, 64), (1, 8))),
        "up_weight": gaussian(key_list[10], (D, FF), D ** -0.5, 0.125, ((0, 64), (1, 8))),
        "down_weight": gaussian(key_list[11], (D, FF), (FF // 4) ** -0.5, 0.15625, ((0, 64), (1, 8))),
    }


norm_eps = 1e-06

def reference(queries, keys, values, in_gate, forget_gate, stream, head_gain, out_weight, norm_gain, gate_weight, up_weight, down_weight):
    blocks = SEQUENCE_TOKENS // BLOCK
    key_scale = HEAD_DIM ** (-0.5)
    cumulative = jnp.cumsum(jax.nn.log_sigmoid(forget_gate).reshape(MEMORY_HEADS, blocks, BLOCK), axis=-1)
    gate_blocks = in_gate.reshape(MEMORY_HEADS, blocks, BLOCK)
    causal = lax.broadcasted_iota(jnp.int32, (BLOCK, BLOCK), 0) >= lax.broadcasted_iota(jnp.int32, (BLOCK, BLOCK), 1)

    def advance(running, section):
        memory, top_now = running
        query_blk, key_blk, value_blk, cum_blk, gate_blk = section
        block_fall = cum_blk[:, -1]
        log_weight = block_fall[:, None] - cum_blk + gate_blk
        block_top = lax.optimization_barrier(jnp.max(log_weight, axis=1))
        key_weight = jnp.exp(log_weight - block_top[:, None]) * key_scale
        weighted = (key_weight.T[:, :, None] * key_blk.astype(jnp.float32)).astype(jnp.bfloat16)
        block_memory = jnp.einsum('shd,she->hde', weighted.astype(jnp.float32), value_blk.astype(jnp.float32))
        spread = cum_blk[:, :, None] - cum_blk[:, None, :] + gate_blk[:, None, :]
        spread = jnp.where(causal, spread, -jnp.inf)
        carried = cum_blk + top_now[:, None]
        row_top = jnp.maximum(carried, lax.optimization_barrier(jnp.max(spread, axis=2)))
        decay_weight = jnp.exp(spread - row_top[:, :, None])
        scores = jnp.einsum('thd,shd->hts', query_blk.astype(jnp.float32), key_blk.astype(jnp.float32))
        weights = (scores * key_scale * decay_weight).astype(jnp.bfloat16)
        inner_part = jnp.einsum('hts,she->the', weights.astype(jnp.float32), value_blk.astype(jnp.float32))
        outer_part = jnp.einsum('thd,hde->the', query_blk.astype(jnp.float32), memory, precision=lax.Precision.HIGHEST)
        readout = jnp.exp(carried - row_top).T[:, :, None] * outer_part + inner_part
        new_top = jnp.maximum(block_fall + top_now, block_top)
        new_memory = jnp.exp(block_fall + top_now - new_top)[:, None, None] * memory + jnp.exp(block_top - new_top)[:, None, None] * block_memory
        return ((new_memory, new_top), readout)

    def split_blocks(array):
        return array.reshape(blocks, BLOCK, MEMORY_HEADS, HEAD_DIM)
    start_state = (jnp.zeros((MEMORY_HEADS, HEAD_DIM, HEAD_DIM), jnp.float32), jnp.zeros((MEMORY_HEADS,), jnp.float32))
    sections = (split_blocks(queries), split_blocks(keys), split_blocks(values), jnp.transpose(cumulative, (1, 0, 2)), jnp.transpose(gate_blocks, (1, 0, 2)))
    final_state, readouts = lax.scan(advance, start_state, sections)
    readouts = readouts.reshape(SEQUENCE_TOKENS, MEMORY_HEADS, HEAD_DIM)
    row_scale = lax.rsqrt(lax.optimization_barrier(jnp.mean(readouts * readouts, axis=-1, keepdims=True)) + norm_eps)
    heads_normed = (readouts * row_scale * head_gain.reshape(MEMORY_HEADS, HEAD_DIM)).astype(jnp.bfloat16).reshape(SEQUENCE_TOKENS, MIX)
    mixed_float = stream.astype(jnp.float32) + jnp.dot(heads_normed, out_weight, preferred_element_type=jnp.float32)
    factor = lax.rsqrt(lax.optimization_barrier(jnp.mean(mixed_float * mixed_float, axis=1, keepdims=True)) + norm_eps)
    normed = (mixed_float * factor * norm_gain).astype(jnp.bfloat16)
    group_width = FF // N_TP

    def channel_rows(row_block):
        gate_acts = jnp.dot(row_block, gate_weight, preferred_element_type=jnp.float32)
        up_acts = jnp.dot(row_block, up_weight, preferred_element_type=jnp.float32)
        hidden = (jax.nn.silu(gate_acts) * up_acts).astype(jnp.bfloat16)
        running_sum = jnp.zeros((row_block.shape[0], D), jnp.float32)
        for group_index in range(N_TP):
            lower = group_index * group_width
            partial_sum = jnp.dot(hidden[:, lower:lower + group_width], down_weight[:, lower:lower + group_width].T, preferred_element_type=jnp.float32)
            rounded = lax.optimization_barrier(partial_sum.astype(jnp.bfloat16))
            running_sum = running_sum + rounded.astype(jnp.float32)
        return running_sum
    channel = lax.map(channel_rows, normed.reshape(SEQUENCE_TOKENS // TOK_DEV, TOK_DEV, D)).reshape(SEQUENCE_TOKENS, D)
    return mixed_float + 0.5 * channel
```

```python
import functools

import jax
import jax.numpy as jnp
from jax import lax
from jax.experimental import pallas as pl
from jax.experimental.pallas import tpu as pltpu
from jax.sharding import Mesh
from jax.sharding import PartitionSpec as P

MESH = pl.DeviceIdType.MESH
F32 = jnp.float32
BF16 = jnp.bfloat16

T = 128
WIDE = 256
UNITS = 176
EPS = 1e-6
FAR = -1e30


def dot(a, b):
    return jnp.dot(a, b, preferred_element_type=F32)


def merge(early, late):
    memory_e, top_e, fall_e = early
    memory_l, top_l, fall_l = late
    top = jnp.maximum(fall_l + top_e, top_l)
    memory = jnp.exp(fall_l + top_e - top) * memory_e + jnp.exp(top_l - top) * memory_l
    return memory, top, fall_e + fall_l


def three_pieces(a):
    high = a.astype(BF16).astype(F32)
    rest = a - high
    middle = rest.astype(BF16).astype(F32)
    return high, middle, rest - middle


def kernel(
    nz,
    ny,
    nx,
    q_ref,
    k_ref,
    v_ref,
    in_ref,
    forget_ref,
    stream_ref,
    head_gain_ref,
    out_w_ref,
    norm_gain_ref,
    gate_w_ref,
    up_w_ref,
    down_w_ref,
    out_ref,
    tail,
    gu_pack,
    d_pack,
    d_block,
    w_gu,
    w_d,
    w_d2,
    m_send,
    m_got,
    z_send,
    z_got,
    e_send,
    e_got,
    heads,
    mixed_ref,
    acts,
    squares,
    hidden,
    r_send,
    r_got,
    ya_s,
    ya_r,
    z_s,
    z_r,
    e_s,
    e_r,
    ring_s,
    ring_r,
    h_s,
    h_r,
    a_s,
    a_r,
    p_s,
    p_r,
    d2_s,
    d2_r,
    x_s,
    x_r,
    r_s,
    r_r,
):
    z, y, x, c = (lax.axis_index(a) for a in ("z", "y", "x", "c"))
    tp = x * 2 + c
    n_tp = 2 * nx
    other = 1 - c

    def remote(src, dst, send, recv, **where):
        return pltpu.make_async_remote_copy(
            src_ref=src,
            dst_ref=dst,
            send_sem=send,
            recv_sem=recv,
            device_id=where,
            device_id_type=MESH,
        )

    def arrived(dst, send, recv):
        remote(dst, dst, send, recv, c=other).wait_recv()

    barrier = pltpu.get_barrier_semaphore()

    def greet(**where):
        pl.semaphore_signal(barrier, inc=1, device_id=where, device_id_type=MESH)

    for dz in range(1, nz):
        greet(z=lax.rem(z + dz, nz))
    plane = [(dx, dy) for dx in range(nx) for dy in range(ny)]
    for dx, dy in plane:
        for dc in range(2):
            if dx or dy or dc:
                greet(x=lax.rem(x + dx, nx), y=lax.rem(y + dy, ny), c=lax.rem(c + dc, 2))

    rows = lax.broadcasted_iota(jnp.int32, (T, T), 0)
    lanes = lax.broadcasted_iota(jnp.int32, (T, T), 1)
    causal = rows >= lanes
    same = rows == lanes
    forget = forget_ref[...]
    fall_each = jnp.minimum(forget, 0.0) - jnp.log1p(jnp.exp(-jnp.abs(forget)))
    in_row = in_ref[...]

    def column(row):
        return jnp.sum(jnp.where(same, jnp.broadcast_to(row, (T, T)), 0.0), axis=1, keepdims=True)

    fall_column = column(fall_each)
    in_column = column(in_row)
    cum_column = jnp.sum(
        jnp.where(causal, jnp.broadcast_to(fall_each, (T, T)), 0.0), axis=1, keepdims=True
    )
    cum_row = jnp.sum(
        jnp.where(rows <= lanes, jnp.broadcast_to(fall_column, (T, T)), 0.0), axis=0, keepdims=True
    )
    fall = jnp.broadcast_to(jnp.sum(fall_each, axis=1, keepdims=True), (1, T))
    log_weight = jnp.broadcast_to(fall - cum_column + in_column, (T, T))
    top = jnp.max(log_weight, axis=0, keepdims=True)
    weighted = jnp.exp(log_weight - top) * (T**-0.5) * k_ref[...].astype(F32)
    memory = lax.dot_general(
        weighted.astype(BF16), v_ref[...], (((0,), (0,)), ((), ())), preferred_element_type=F32
    )
    slice_rows = T // ny
    sub8 = lax.broadcasted_iota(jnp.int32, (8, T), 0)
    for j in range(ny):
        m_send[j, 0:slice_rows] = memory[j * slice_rows : (j + 1) * slice_rows]
        m_send[j, slice_rows : slice_rows + 8] = jnp.where(
            sub8 == 0, top, jnp.where(sub8 == 1, fall, 0.0)
        )
    m_got[y] = m_send[y]

    shard = gate_w_ref.shape[0]
    lane = lax.broadcasted_iota(jnp.int32, (shard, T), 1)
    ends = []
    for n, ref in enumerate((gate_w_ref, up_w_ref, down_w_ref)):
        tail[n] = jnp.zeros((shard, T), F32)
        tail[n, :, 0:64] = ref[:, 640:704].astype(F32)
        ends.append((ref[:, 512:640].astype(F32), tail[n]))

    def rest_of(n, j, at):
        wide, narrow = ends[n]
        wide = pltpu.roll(wide, (at - 32 * j) % T, 1)
        narrow = pltpu.roll(narrow, (at + 32 - 16 * j) % T, 1)
        here = (lane >= at) & (lane < at + 48)
        return jnp.where(here, jnp.where(lane < at + 32, wide, narrow), 0.0)

    for j in range(ny):
        gu_pack[j, :, 0:128] = gate_w_ref[:, j * T : (j + 1) * T]
        gu_pack[j, :, 128:256] = up_w_ref[:, j * T : (j + 1) * T]
        gu_pack[j, :, 256:384] = (rest_of(0, j, 0) + rest_of(1, j, 64)).astype(BF16)
        d_pack[j, :, 0:128] = down_w_ref[:, j * T : (j + 1) * T]
        d_pack[j, :, 128:256] = rest_of(2, j, 0).astype(BF16)

    def gu_rows(slot, begin, count):
        return w_gu.at[slot // 2, pl.ds(pl.multiple_of((slot % 2) * T + begin, 32), count), :]

    own_rows = pl.ds(pl.multiple_of((z % 2) * T + y * shard, 32), shard)
    w_gu[z // 2, own_rows, :] = gu_pack[y]
    d_block[pl.ds(pl.multiple_of(y * shard, 32), shard), :] = d_pack[y]
    for s in range(nz):
        w_d[s, UNITS:256] = jnp.zeros((256 - UNITS, T), BF16)
    for s in range(nz // 2):
        w_d2[s, UNITS:256] = jnp.zeros((256 - UNITS, T), BF16)

    pl.semaphore_wait(barrier, nz - 1 + 2 * nx * ny - 1)

    sent = []

    def send(*args, **where):
        copy = remote(*args, **where)
        copy.start()
        sent.append(copy)

    for dy in range(1, ny):
        to = lax.rem(y + dy, ny)
        send(m_send.at[to], m_got.at[y], ya_s.at[0, dy], ya_r.at[0, dy], y=to)
    for dy in range(1, ny):
        to = lax.rem(y + dy, ny)
        send(gu_pack.at[to], gu_rows(z, y * shard, shard), ya_s.at[1, dy], ya_r.at[1, dy], y=to)
        d_rows = pl.ds(pl.multiple_of(y * shard, 32), shard)
        send(d_pack.at[to], d_block.at[d_rows], ya_s.at[2, dy], ya_r.at[2, dy], y=to)

    scores = lax.dot_general(
        q_ref[...], k_ref[...], (((1,), (1,)), ((), ())), preferred_element_type=F32
    ) * (T**-0.5)

    for dy in range(1, ny):
        arrived(m_got.at[lax.rem(y + ny - dy, ny)], ya_s.at[0, dy], ya_r.at[0, dy])
    state = (jnp.zeros((slice_rows, T), F32), jnp.full((1, T), FAR, F32), jnp.zeros((1, T), F32))
    before = []
    for j in range(ny):
        before.append(state)
        got = m_got[j]
        late = (
            got[0:slice_rows],
            got[slice_rows : slice_rows + 1],
            got[slice_rows + 1 : slice_rows + 2],
        )
        state = merge(state, late)
    plane_memory, plane_top, plane_fall = state
    sub16 = lax.broadcasted_iota(jnp.int32, (16, T), 0)
    numbers = jnp.zeros((16, T), F32)
    for n, piece in enumerate((*three_pieces(plane_top), *three_pieces(plane_fall))):
        numbers = jnp.where(sub16 == n, piece, numbers)
    z_send[0:slice_rows] = plane_memory.astype(BF16)
    z_send[slice_rows : slice_rows + 16] = numbers.astype(BF16)
    for dz in range(nz - 1, 0, -1):

        @pl.when(z + dz < nz)
        def _():
            remote(z_send, z_got.at[dz], z_s.at[dz], z_r.at[dz], z=z + dz).start()

    up_z, down_z = lax.rem(z + 1, nz), lax.rem(z + nz - 1, nz)
    rounds = nz // 2

    def ring_parts(n, slot, r, **where):
        return (
            remote(
                gu_rows(slot, 0, T),
                gu_rows(slot, 0, T),
                ring_s.at[n, 0, r],
                ring_r.at[n, 0, r],
                **where,
            ),
            remote(
                w_d.at[slot, pl.ds(0, UNITS)],
                w_d.at[slot, pl.ds(0, UNITS)],
                ring_s.at[n, 1, r],
                ring_r.at[n, 1, r],
                **where,
            ),
        )

    def ring_start(r):
        for copy in ring_parts(0, lax.rem(z + nz - r + 1, nz), r, z=up_z):
            copy.start()
            sent.append(copy)
        if r < rounds:
            for copy in ring_parts(1, lax.rem(z + r - 1, nz), r, z=down_z):
                copy.start()
                sent.append(copy)

    def ring_wait(r):
        for copy in ring_parts(0, lax.rem(z + nz - r, nz), r, z=up_z):
            copy.wait_recv()
        if r < rounds:
            for copy in ring_parts(1, lax.rem(z + r, nz), r, z=down_z):
                copy.wait_recv()

    def ring_turn(r):
        ring_wait(r)
        if r < rounds:
            ring_start(r + 1)

    for dy in range(1, ny):
        by = lax.rem(y + ny - dy, ny)
        arrived(gu_rows(z, by * shard, shard), ya_s.at[1, dy], ya_r.at[1, dy])
        d_rows = pl.ds(pl.multiple_of(by * shard, 32), shard)
        arrived(d_block.at[d_rows], ya_s.at[2, dy], ya_r.at[2, dy])
    turned = jnp.transpose(d_block[...].astype(F32))
    w_d[z, 0:UNITS] = turned[0:UNITS].astype(BF16)
    ring_start(1)

    def pass_plane(dz, carry):
        total, highest, fallen = carry
        arrived(z_got.at[dz], z_s.at[dz], z_r.at[dz])
        got = z_got[dz].astype(F32)
        found = got[slice_rows : slice_rows + 16]
        top_there = found[0:1] + found[1:2] + found[2:3]
        fall_there = found[3:4] + found[4:5] + found[5:6]
        level = top_there + fallen
        new = jnp.maximum(highest, level)
        total = total * jnp.exp(highest - new) + jnp.exp(level - new) * got[0:slice_rows]
        return total, new, fallen + fall_there

    total, highest, fallen = lax.fori_loop(
        1,
        z + 1,
        pass_plane,
        (jnp.zeros((slice_rows, T), F32), jnp.full((1, T), FAR, F32), jnp.zeros((1, T), F32)),
    )
    top_in = jnp.maximum(fallen, highest)
    plane_in = (total * jnp.exp(highest - top_in), top_in, jnp.zeros((1, T), F32))
    for j in range(ny):
        memory_j, top_j, _ = merge(plane_in, before[j])
        e_send[j, 0:slice_rows] = memory_j
        e_send[j, slice_rows : slice_rows + 8] = jnp.broadcast_to(top_j, (8, T))
    e_got[y] = e_send[y]
    for dy in range(1, ny):
        to = lax.rem(y + dy, ny)
        send(e_send.at[to], e_got.at[y], e_s.at[dy], e_r.at[dy], y=to)

    ring_turn(1)

    for dy in range(1, ny):
        arrived(e_got.at[lax.rem(y + ny - dy, ny)], e_s.at[dy], e_r.at[dy])

    memory_in = jnp.concatenate([e_got[j, 0:slice_rows] for j in range(ny)], axis=0)
    top_here = e_got[0, slice_rows : slice_rows + 1]
    cum_wide = jnp.broadcast_to(cum_column, (T, T))
    carried = cum_wide + top_here
    spread = jnp.where(causal, cum_wide - cum_row + in_row, -jnp.inf)
    row_top = jnp.maximum(carried, jnp.max(spread, axis=1, keepdims=True))
    block_weights = (scores * jnp.exp(spread - row_top)).astype(BF16)
    inner = dot(block_weights, v_ref[...])
    outer = sum(dot(q_ref[...], piece.astype(BF16)) for piece in three_pieces(memory_in))
    readout = jnp.exp(carried - row_top) * outer + inner
    scale = lax.rsqrt(jnp.mean(readout * readout, axis=1, keepdims=True) + EPS)
    normed_heads = (readout * scale * head_gain_ref[pl.ds(tp, 1), :]).astype(BF16)
    heads[tp] = normed_heads
    for d in range(1, n_tp):
        to = lax.rem(tp + d, n_tp)
        send(heads.at[tp], heads.at[tp], h_s.at[d], h_r.at[d], x=to // 2, c=to % 2)

    ring_turn(2)

    for d in range(1, n_tp):
        by = lax.rem(tp + n_tp - d, n_tp)
        arrived(heads.at[by], h_s.at[d], h_r.at[d])
    mixed = stream_ref[...].astype(F32)
    for n in range(nx):
        pair = jnp.concatenate([heads[2 * n], heads[2 * n + 1]], axis=1)
        mixed = mixed + dot(pair, out_w_ref[n * WIDE : (n + 1) * WIDE, :])
    mixed_ref[...] = mixed
    own_tokens = pl.ds(pl.multiple_of(y * T, T), T)
    for half in range(2):
        gain = norm_gain_ref[pl.ds(2 * tp + half, 1), :]
        part = mixed[:, half * T : (half + 1) * T]
        acts[tp, own_tokens, half * T : (half + 1) * T] = (part * gain).astype(BF16)
    square_column = jnp.sum(mixed * mixed, axis=1, keepdims=True)
    square_row = jnp.sum(
        jnp.where(same, jnp.broadcast_to(square_column, (T, T)), 0.0), axis=0, keepdims=True
    )
    squares[tp, y] = jnp.broadcast_to(square_row, (8, T))

    def piece_of(tp_there, y_there):
        tokens = pl.ds(pl.multiple_of(y_there * T, T), T)
        return acts.at[tp_there, tokens, :], squares.at[tp_there, y_there]

    def pass_on(n):
        dx, dy = plane[n]
        tp_there = lax.rem(x + nx - dx, nx) * 2 + c
        for m, ref in enumerate(piece_of(tp_there, lax.rem(y + ny - dy, ny))):
            send(ref, ref, p_s.at[m, n], p_r.at[m, n], c=other)

    order = sorted(
        range(1, len(plane)), key=lambda n: sum(min(d, 4 - d) for d in plane[n])
    )
    for n in reversed(order):
        dx, dy = plane[n]
        for m, ref in enumerate(piece_of(tp, y)):
            send(
                ref,
                ref,
                a_s.at[m, n],
                a_r.at[m, n],
                x=lax.rem(x + dx, nx),
                y=lax.rem(y + dy, ny),
            )
    pass_on(0)
    for r in range(3, rounds + 1):
        ring_turn(r)

    for b in range(nx):
        for half in range(2):
            send(
                w_d.at[4 * b + 2 * other + half, pl.ds(0, UNITS)],
                w_d2.at[2 * b + half, pl.ds(0, UNITS)],
                d2_s.at[2 * b + half],
                d2_r.at[2 * b + half],
                c=other,
            )

    for n in order:
        dx, dy = plane[n]
        tp_there = lax.rem(x + nx - dx, nx) * 2 + c
        for m, ref in enumerate(piece_of(tp_there, lax.rem(y + ny - dy, ny))):
            arrived(ref, a_s.at[m, n], a_r.at[m, n])
        pass_on(n)
    for n in range(len(plane)):
        dx, dy = plane[n]
        tp_there = lax.rem(x + nx - dx, nx) * 2 + other
        for m, ref in enumerate(piece_of(tp_there, lax.rem(y + ny - dy, ny))):
            arrived(ref, p_s.at[m, n], p_r.at[m, n])

    lane_wide = lax.broadcasted_iota(jnp.int32, (T, T), 1)
    for j in range(ny):
        both = jnp.zeros((T, 3 * T), F32)
        total_square = jnp.zeros((1, T), F32)
        for b in range(n_tp):
            both = both + dot(acts[b, j * T : (j + 1) * T, :], w_gu[b])
            total_square = total_square + squares[b, j][0:1]
        factor = lax.rsqrt(column(total_square) * (1.0 / (n_tp * WIDE)) + EPS)
        both = both * factor
        gate, up, rest = both[:, 0:T], both[:, T : 2 * T], both[:, 2 * T : 3 * T]
        hidden[c, j * T : (j + 1) * T, 0:T] = (gate / (1.0 + jnp.exp(-gate)) * up).astype(BF16)
        small = rest / (1.0 + jnp.exp(-rest)) * pltpu.roll(rest, 64, 1)
        hidden[c, j * T : (j + 1) * T, T : 2 * T] = jnp.where(lane_wide < 48, small, 0.0).astype(
            BF16
        )
    send(hidden.at[c], hidden.at[c], x_s, x_r, c=other)

    for n in range(2 * nx):
        arrived(w_d2.at[n, pl.ds(0, UNITS)], d2_s.at[n], d2_r.at[n])
    arrived(hidden.at[other], x_s, x_r)

    for dx in (2, 1, 3, 0):
        b = lax.rem(x + dx, nx)
        own = jnp.concatenate([w_d[4 * b + 2 * c], w_d[4 * b + 2 * c + 1]], axis=1)
        theirs = jnp.concatenate([w_d2[2 * b], w_d2[2 * b + 1]], axis=1)
        r_send[dx] = (dot(hidden[c], own) + dot(hidden[other], theirs)).astype(BF16)
        for dy in (2, 1, 3, 0):
            if dx or dy:
                to = lax.rem(y + dy, ny)
                send(
                    r_send.at[dx, pl.ds(pl.multiple_of(to * T, T), T), :],
                    r_got.at[dx * ny + dy],
                    r_s.at[dx * ny + dy],
                    r_r.at[dx * ny + dy],
                    x=b,
                    y=to,
                )
    channel = r_send[0, own_tokens, :].astype(F32)
    for n in order:
        arrived(r_got.at[n], r_s.at[n], r_r.at[n])
        channel = channel + r_got[n].astype(F32)
    out_ref[...] = mixed_ref[...] + 0.5 * channel

    for dz in range(1, nz):

        @pl.when(z + dz < nz)
        def _():
            remote(z_send, z_got.at[dz], z_s.at[dz], z_r.at[dz], z=z + dz).wait_send()

    for copy in sent:
        copy.wait_send()


def local(nz, ny, nx, *args):
    queries, keys, values, in_gate, forget_gate, stream = args[:6]
    head_gain, out_weight, norm_gain, gate_weight, up_weight, down_weight = args[6:]
    n_tp = 2 * nx
    dma = pltpu.SemaphoreType.DMA
    vmem = pltpu.VMEM
    slice_rows = T // ny
    shard = gate_weight.shape[0]
    scratch = [
        vmem((3, shard, T), F32),
        vmem((ny, shard, 3 * T), BF16),
        vmem((ny, shard, 2 * T), BF16),
        vmem((T, 2 * T), BF16),
        vmem((nz // 2, 2 * T, 3 * T), BF16),
        vmem((nz, 256, T), BF16),
        vmem((nz // 2, 256, T), BF16),
        vmem((ny, slice_rows + 8, T), F32),
        vmem((ny, slice_rows + 8, T), F32),
        vmem((slice_rows + 16, T), BF16),
        vmem((nz, slice_rows + 16, T), BF16),
        vmem((ny, slice_rows + 8, T), F32),
        vmem((ny, slice_rows + 8, T), F32),
        vmem((n_tp, T, T), BF16),
        vmem((T, WIDE), F32),
        vmem((n_tp, ny * T, WIDE), BF16),
        vmem((n_tp, ny, 8, T), F32),
        vmem((2, ny * T, 2 * T), BF16),
        vmem((nx, ny * T, WIDE), BF16),
        vmem((nx * ny, T, WIDE), BF16),
    ]
    for shape in (
        (3, ny),
        (nz,),
        (ny,),
        (2, 2, nz // 2 + 1),
        (n_tp,),
        (2, nx * ny),
        (2, nx * ny),
        (2 * nx,),
        None,
        (nx * ny,),
    ):
        scratch += [dma if shape is None else dma(shape)] * 2
    return pl.pallas_call(
        functools.partial(kernel, nz, ny, nx),
        out_shape=jax.ShapeDtypeStruct((T, WIDE), F32),
        in_specs=[pl.BlockSpec(memory_space=vmem)] * 12,
        out_specs=pl.BlockSpec(memory_space=vmem),
        scratch_shapes=scratch,
        compiler_params=pltpu.CompilerParams(collective_id=0, has_side_effects=True),
        name="layer",
    )(
        queries,
        keys,
        values,
        in_gate,
        forget_gate,
        stream,
        head_gain.reshape(n_tp, T),
        out_weight,
        norm_gain.reshape(2 * n_tp, T),
        gate_weight,
        up_weight,
        down_weight,
    )


def solution(mesh):
    nz, ny, nx = 16, 4, mesh.shape["tp"] // 2
    finer = Mesh(mesh.devices.reshape(nz, ny, nx, 2), ("z", "y", "x", "c"))
    rows, columns = ("z", "y"), ("x", "c")
    in_specs = (
        P(rows, columns),
        P(rows, columns),
        P(rows, columns),
        P(columns, rows),
        P(columns, rows),
        P(rows, columns),
        P(),
        P(None, columns),
        P(),
        P(rows, columns),
        P(rows, columns),
        P(rows, columns),
    )
    return jax.shard_map(
        functools.partial(local, nz, ny, nx),
        mesh=finer,
        in_specs=in_specs,
        out_specs=P(rows, columns),
        check_vma=False,
    )
```

```python
import functools

import jax
import jax.numpy as jnp
from jax import lax
from jax.experimental import pallas as pl
from jax.experimental.pallas import tpu as pltpu
from jax.sharding import Mesh
from jax.sharding import PartitionSpec as P

MESH = pl.DeviceIdType.MESH
F32 = jnp.float32
BF16 = jnp.bfloat16

T = 128
WIDE = 256
UNITS = 176
EPS = 1e-6
FAR = -1e30
SECTION = 4
TURNS = ((1, 1), (6, 6), (3, 3), (3, 3))
GROUPS = (2, 1, 3, 0)
RING_ROUNDS = (8, 7)


def dot(a, b):
    return jnp.dot(a, b, preferred_element_type=F32)


def merge(early, late):
    memory_e, top_e, fall_e = early
    memory_l, top_l, fall_l = late
    top = jnp.maximum(fall_l + top_e, top_l)
    memory = jnp.exp(fall_l + top_e - top) * memory_e + jnp.exp(top_l - top) * memory_l
    return memory, top, fall_e + fall_l


def three_pieces(a):
    high = a.astype(BF16).astype(F32)
    rest = a - high
    middle = rest.astype(BF16).astype(F32)
    return high, middle, rest - middle


def kernel(
    nz,
    ny,
    nx,
    q_ref,
    k_ref,
    v_ref,
    in_ref,
    forget_ref,
    stream_ref,
    head_gain_ref,
    out_w_ref,
    norm_gain_ref,
    gate_w_ref,
    up_w_ref,
    down_w_ref,
    out_ref,
    tail,
    gu_pack,
    d_pack,
    d_block,
    w_gu,
    w_d,
    w_d2,
    m_send,
    m_got,
    z_send,
    z_got,
    s_send,
    s_got,
    e_send,
    e_got,
    heads,
    mixed_ref,
    acts,
    squares,
    hidden,
    r_send,
    r_got,
    ya_s,
    ya_r,
    z_s,
    z_r,
    s_s,
    s_r,
    e_s,
    e_r,
    ring_s,
    ring_r,
    h_s,
    h_r,
    a_s,
    a_r,
    p_s,
    p_r,
    d2_s,
    d2_r,
    x_s,
    x_r,
    r_s,
    r_r,
):
    z, y, x, c = (lax.axis_index(a) for a in ("z", "y", "x", "c"))
    tp = x * 2 + c
    n_tp = 2 * nx
    other = 1 - c

    def remote(src, dst, send, recv, **where):
        return pltpu.make_async_remote_copy(
            src_ref=src,
            dst_ref=dst,
            send_sem=send,
            recv_sem=recv,
            device_id=where,
            device_id_type=MESH,
        )

    def arrived(dst, send, recv):
        remote(dst, dst, send, recv, c=other).wait_recv()

    barrier = pltpu.get_barrier_semaphore()

    def greet(**where):
        pl.semaphore_signal(barrier, inc=1, device_id=where, device_id_type=MESH)

    for dz in range(1, nz):
        greet(z=lax.rem(z + dz, nz))
    plane = [(dx, dy) for dx in range(nx) for dy in range(ny)]
    for dx, dy in plane:
        for dc in range(2):
            if dx or dy or dc:
                greet(x=lax.rem(x + dx, nx), y=lax.rem(y + dy, ny), c=lax.rem(c + dc, 2))

    rows = lax.broadcasted_iota(jnp.int32, (T, T), 0)
    lanes = lax.broadcasted_iota(jnp.int32, (T, T), 1)
    causal = rows >= lanes
    same = rows == lanes
    forget = forget_ref[...]
    fall_each = jnp.minimum(forget, 0.0) - jnp.log1p(jnp.exp(-jnp.abs(forget)))
    in_row = in_ref[...]

    def column(row):
        return jnp.sum(jnp.where(same, jnp.broadcast_to(row, (T, T)), 0.0), axis=1, keepdims=True)

    fall_column = column(fall_each)
    in_column = column(in_row)
    cum_column = jnp.sum(
        jnp.where(causal, jnp.broadcast_to(fall_each, (T, T)), 0.0), axis=1, keepdims=True
    )
    cum_row = jnp.sum(
        jnp.where(rows <= lanes, jnp.broadcast_to(fall_column, (T, T)), 0.0), axis=0, keepdims=True
    )
    fall = jnp.broadcast_to(jnp.sum(fall_each, axis=1, keepdims=True), (1, T))
    log_weight = jnp.broadcast_to(fall - cum_column + in_column, (T, T))
    top = jnp.max(log_weight, axis=0, keepdims=True)
    weighted = jnp.exp(log_weight - top) * (T**-0.5) * k_ref[...].astype(F32)
    memory = lax.dot_general(
        weighted.astype(BF16), v_ref[...], (((0,), (0,)), ((), ())), preferred_element_type=F32
    )
    slice_rows = T // ny
    sub8 = lax.broadcasted_iota(jnp.int32, (8, T), 0)
    for j in range(ny):
        m_send[j, 0:slice_rows] = memory[j * slice_rows : (j + 1) * slice_rows]
        m_send[j, slice_rows : slice_rows + 8] = jnp.where(
            sub8 == 0, top, jnp.where(sub8 == 1, fall, 0.0)
        )
    m_got[y] = m_send[y]

    shard = gate_w_ref.shape[0]
    lane = lax.broadcasted_iota(jnp.int32, (shard, T), 1)
    ends = []
    for n, ref in enumerate((gate_w_ref, up_w_ref, down_w_ref)):
        tail[n] = jnp.zeros((shard, T), F32)
        tail[n, :, 0:64] = ref[:, 640:704].astype(F32)
        ends.append((ref[:, 512:640].astype(F32), tail[n]))

    def rest_of(n, j, at):
        wide, narrow = ends[n]
        wide = pltpu.roll(wide, (at - 32 * j) % T, 1)
        narrow = pltpu.roll(narrow, (at + 32 - 16 * j) % T, 1)
        here = (lane >= at) & (lane < at + 48)
        return jnp.where(here, jnp.where(lane < at + 32, wide, narrow), 0.0)

    for j in range(ny):
        gu_pack[j, :, 0:128] = gate_w_ref[:, j * T : (j + 1) * T]
        gu_pack[j, :, 128:256] = up_w_ref[:, j * T : (j + 1) * T]
        gu_pack[j, :, 256:384] = (rest_of(0, j, 0) + rest_of(1, j, 64)).astype(BF16)
        d_pack[j, :, 0:128] = down_w_ref[:, j * T : (j + 1) * T]
        d_pack[j, :, 128:256] = rest_of(2, j, 0).astype(BF16)

    def gu_rows(slot, begin, count):
        return w_gu.at[slot, pl.ds(pl.multiple_of(begin, 32), count), :]

    w_gu[z, pl.ds(pl.multiple_of(y * shard, 32), shard), :] = gu_pack[y]
    d_block[pl.ds(pl.multiple_of(y * shard, 32), shard), :] = d_pack[y]
    for s in range(nz):
        w_d[s, UNITS:256] = jnp.zeros((256 - UNITS, T), BF16)
    for s in range(nz // 2):
        w_d2[s, UNITS:256] = jnp.zeros((256 - UNITS, T), BF16)

    pl.semaphore_wait(barrier, nz - 1 + 2 * nx * ny - 1)

    def send(*args, **where):
        remote(*args, **where).start()

    for dy in range(1, ny):
        to = lax.rem(y + dy, ny)
        send(m_send.at[to], m_got.at[y], ya_s.at[0], ya_r.at[0], y=to)
    for dy in range(1, ny):
        to = lax.rem(y + dy, ny)
        send(gu_pack.at[to], gu_rows(z, y * shard, shard), ya_s.at[1], ya_r.at[1], y=to)
        d_rows = pl.ds(pl.multiple_of(y * shard, 32), shard)
        send(d_pack.at[to], d_block.at[d_rows], ya_s.at[2], ya_r.at[2], y=to)

    scores = lax.dot_general(
        q_ref[...], k_ref[...], (((1,), (1,)), ((), ())), preferred_element_type=F32
    ) * (T**-0.5)

    arrived(m_got.at[0 : ny - 1], ya_s.at[0], ya_r.at[0])
    state = (jnp.zeros((slice_rows, T), F32), jnp.full((1, T), FAR, F32), jnp.zeros((1, T), F32))
    before = []
    for j in range(ny):
        before.append(state)
        got = m_got[j]
        late = (
            got[0:slice_rows],
            got[slice_rows : slice_rows + 1],
            got[slice_rows + 1 : slice_rows + 2],
        )
        state = merge(state, late)
    plane_memory, plane_top, plane_fall = state

    def packed(memory, top, fall):
        numbers = jnp.zeros((8, T), F32)
        for n, piece in enumerate((*three_pieces(top), *three_pieces(fall))):
            numbers = jnp.where(sub8 == n, piece, numbers)
        return jnp.concatenate([memory, numbers], axis=0).astype(BF16)

    section, place = z // SECTION, lax.rem(z, SECTION)
    z_send[...] = packed(plane_memory, plane_top, plane_fall)

    def plane_part(dz):
        return remote(z_send, z_got.at[dz], z_s.at[dz], z_r.at[dz], z=z + dz)

    def section_part(dz):
        return remote(s_send, s_got.at[section], s_s.at[dz], s_r.at[section], z=z + dz)

    def to_planes(act):
        for dz in range(SECTION - 1, 0, -1):
            pl.when(place + dz < SECTION)(functools.partial(act, plane_part(dz)))

    def to_sections(act):
        for dz in range(nz - SECTION, 0, -1):
            due = (place == SECTION - 1) & (z + dz < nz)
            pl.when(due)(functools.partial(act, section_part(dz)))

    to_planes(lambda copy: copy.start())

    up_z, down_z = lax.rem(z + 1, nz), lax.rem(z + nz - 1, nz)
    rounds = RING_ROUNDS

    def ring_part(way, r, m, arriving):
        step = r if arriving else r - 1
        slot = lax.rem(z + step, nz) if way else lax.rem(z + nz - step, nz)
        ref = w_d.at[slot, pl.ds(0, UNITS)] if m == 2 else gu_rows(slot, m * (T // 2), T // 2)
        to = down_z if way else up_z
        return remote(ref, ref, ring_s.at[2 * way + m // 2], ring_r.at[way, m, r], z=to)

    def lend(slot):
        @pl.when(lax.rem(slot // 2, 2) == other)
        def _():
            there = w_d2.at[2 * (slot // 4) + lax.rem(slot, 2), pl.ds(0, UNITS)]
            send(w_d.at[slot, pl.ds(0, UNITS)], there, d2_s, d2_r, c=other)

    def ring_begin(way):
        for m in range(3):
            ring_part(way, 1, m, False).start()

    turns = [[(r, m) for r in range(1, rounds[way] + 1) for m in range(3)] for way in range(2)]

    def ring_turns(way, count):
        for r, m in turns[way][:count]:
            ring_part(way, r, m, True).wait_recv()
            if r < rounds[way]:
                ring_part(way, r + 1, m, False).start()
            if m == 2:
                lend(lax.rem(z + r, nz) if way else lax.rem(z + nz - r, nz))
        del turns[way][:count]

    def both_turns(up, down):
        for n in range(max(up, down)):
            if n < up:
                ring_turns(0, 1)
            if n < down:
                ring_turns(1, 1)

    arrived(gu_pack.at[0 : ny - 1], ya_s.at[1], ya_r.at[1])
    arrived(d_pack.at[0 : ny - 1], ya_s.at[2], ya_r.at[2])
    turned = jnp.transpose(d_block[...].astype(F32))
    w_d[z, 0:UNITS] = turned[0:UNITS].astype(BF16)

    def passing(carry, got):
        total, highest, fallen = carry
        got = got.astype(F32)
        found = got[slice_rows : slice_rows + 8]
        level = found[0:1] + found[1:2] + found[2:3] + fallen
        new = jnp.maximum(highest, level)
        total = total * jnp.exp(highest - new) + jnp.exp(level - new) * got[0:slice_rows]
        return total, new, fallen + (found[3:4] + found[4:5] + found[5:6])

    def pass_plane(dz, carry):
        arrived(z_got.at[dz], z_s.at[dz], z_r.at[dz])
        return passing(carry, z_got[dz])

    def pass_section(n, carry):
        n = section - 1 - n
        arrived(s_got.at[n], s_s.at[0], s_r.at[n])
        return passing(carry, s_got[n])

    ring_begin(0)
    ring_begin(1)
    lend(z)
    both_turns(*TURNS[0])
    passed = (jnp.zeros((slice_rows, T), F32), jnp.full((1, T), FAR, F32), jnp.zeros((1, T), F32))
    passed = lax.fori_loop(1, place + 1, pass_plane, passed)
    s_send[...] = packed(*merge(passed, (plane_memory, plane_top, plane_fall)))
    to_sections(lambda copy: copy.start())
    both_turns(*TURNS[1])
    total, highest, fallen = lax.fori_loop(0, section, pass_section, passed)
    top_in = jnp.maximum(fallen, highest)
    plane_in = (total * jnp.exp(highest - top_in), top_in, jnp.zeros((1, T), F32))
    for j in range(ny):
        memory_j, top_j, _ = merge(plane_in, before[j])
        e_send[j, 0:slice_rows] = memory_j
        e_send[j, slice_rows : slice_rows + 8] = jnp.broadcast_to(top_j, (8, T))
    e_got[y] = e_send[y]
    for dy in range(1, ny):
        to = lax.rem(y + dy, ny)
        send(e_send.at[to], e_got.at[y], e_s, e_r, y=to)
    both_turns(*TURNS[2])
    arrived(e_got.at[0 : ny - 1], e_s, e_r)

    memory_in = jnp.concatenate([e_got[j, 0:slice_rows] for j in range(ny)], axis=0)
    top_here = e_got[0, slice_rows : slice_rows + 1]
    cum_wide = jnp.broadcast_to(cum_column, (T, T))
    carried = cum_wide + top_here
    spread = jnp.where(causal, cum_wide - cum_row + in_row, -jnp.inf)
    row_top = jnp.maximum(carried, jnp.max(spread, axis=1, keepdims=True))
    block_weights = (scores * jnp.exp(spread - row_top)).astype(BF16)
    inner = dot(block_weights, v_ref[...])
    outer = sum(dot(q_ref[...], piece.astype(BF16)) for piece in three_pieces(memory_in))
    readout = jnp.exp(carried - row_top) * outer + inner
    scale = lax.rsqrt(jnp.mean(readout * readout, axis=1, keepdims=True) + EPS)
    normed_heads = (readout * scale * head_gain_ref[pl.ds(tp, 1), :]).astype(BF16)
    heads[tp] = normed_heads
    for d in range(1, n_tp):
        to = lax.rem(tp + d, n_tp)
        send(heads.at[tp], heads.at[tp], h_s, h_r, x=to // 2, c=to % 2)

    both_turns(*TURNS[3])

    arrived(heads.at[0 : n_tp - 1], h_s, h_r)
    mixed = stream_ref[...].astype(F32)
    for n in range(nx):
        pair = jnp.concatenate([heads[2 * n], heads[2 * n + 1]], axis=1)
        mixed = mixed + dot(pair, out_w_ref[n * WIDE : (n + 1) * WIDE, :])
    mixed_ref[...] = mixed
    own_tokens = pl.ds(pl.multiple_of(y * T, T), T)
    for half in range(2):
        gain = norm_gain_ref[pl.ds(2 * tp + half, 1), :]
        part = mixed[:, half * T : (half + 1) * T]
        acts[tp, own_tokens, half * T : (half + 1) * T] = (part * gain).astype(BF16)
    square_column = jnp.sum(mixed * mixed, axis=1, keepdims=True)
    square_row = jnp.sum(
        jnp.where(same, jnp.broadcast_to(square_column, (T, T)), 0.0), axis=0, keepdims=True
    )
    squares[tp * ny + y] = jnp.broadcast_to(square_row, (8, T))

    def piece_of(tp_there, y_there):
        tokens = pl.ds(pl.multiple_of(y_there * T, T), T)
        return acts.at[tp_there, tokens, :], squares.at[tp_there * ny + y_there]

    def pass_on(dy, dxs):
        for dx in dxs:
            tp_there = lax.rem(x + nx - dx, nx) * 2 + c
            for m, ref in enumerate(piece_of(tp_there, lax.rem(y + ny - dy, ny))):
                send(ref, ref, p_s.at[m], p_r.at[m, dy], c=other)

    for dy in GROUPS:
        for dx in GROUPS:
            if dx or dy:
                for m, ref in enumerate(piece_of(tp, y)):
                    there = dict(x=lax.rem(x + dx, nx), y=lax.rem(y + dy, ny))
                    send(ref, ref, a_s.at[m], a_r.at[m, dy], **there)
    pass_on(0, (0,))

    both_turns(len(turns[0]), len(turns[1]))
    for dy in GROUPS:
        dxs = [dx for dx in GROUPS if dx or dy]
        arrived(r_got.at[0 : len(dxs)], a_s.at[0], a_r.at[0, dy])
        arrived(squares.at[0 : len(dxs)], a_s.at[1], a_r.at[1, dy])
        pass_on(dy, dxs)

    lane_wide = lax.broadcasted_iota(jnp.int32, (T, T), 1)

    def tokens_of(dy):
        return pl.ds(pl.multiple_of(lax.rem(y + ny - dy, ny) * T, T), T)

    def make_hidden(n):
        dy = GROUPS[n]
        arrived(r_got.at[0:nx], p_s.at[0], p_r.at[0, dy])
        arrived(squares.at[0:nx], p_s.at[1], p_r.at[1, dy])
        tokens = tokens_of(dy)
        total_square = jnp.zeros((1, T), F32)
        both = jnp.zeros((T, 3 * T), F32)
        for b in range(n_tp):
            total_square = total_square + squares[b * ny + lax.rem(y + ny - dy, ny)][0:1]
            both = both + dot(acts[b, tokens, :], w_gu[2 * b : 2 * b + 2].reshape(2 * T, 3 * T))
        factor = lax.rsqrt(column(total_square) * (1.0 / (n_tp * WIDE)) + EPS)
        both = both * factor
        gate, up, rest = both[:, 0:T], both[:, T : 2 * T], both[:, 2 * T : 3 * T]
        here = slice(n * T, (n + 1) * T)
        hidden[c, here, 0:T] = (gate / (1.0 + jnp.exp(-gate)) * up).astype(BF16)
        small = rest / (1.0 + jnp.exp(-rest)) * pltpu.roll(rest, 64, 1)
        hidden[c, here, T : 2 * T] = jnp.where(lane_wide < 48, small, 0.0).astype(BF16)
        ref = hidden.at[c, here, :]
        send(ref, ref, x_s, x_r.at[n], c=other)

    def share_out(first, last):
        for n in range(first, last):
            arrived(hidden.at[other, n * T : (n + 1) * T, :], x_s, x_r.at[n])
        mine, partners = (hidden[core, first * T : last * T, :] for core in (c, other))
        for dx in GROUPS:
            b = lax.rem(x + nx - dx, nx)
            own = jnp.concatenate([w_d[4 * b + 2 * c], w_d[4 * b + 2 * c + 1]], axis=1)
            theirs = jnp.concatenate([w_d2[2 * b], w_d2[2 * b + 1]], axis=1)
            share = (dot(mine, own) + dot(partners, theirs)).astype(BF16)
            for n in range(first, last):
                dy = GROUPS[n]
                to = dx * ny + dy
                r_send[to] = share[(n - first) * T : (n - first + 1) * T]
                if to:
                    there = dict(x=b, y=lax.rem(y + ny - dy, ny))
                    send(r_send.at[to], r_got.at[to], r_s, r_r.at[dy], **there)

    make_hidden(0)
    make_hidden(1)
    arrived(w_d2.at[0 : 2 * nx, pl.ds(0, UNITS)], d2_s, d2_r)
    share_out(0, 1)
    make_hidden(2)
    make_hidden(3)
    share_out(1, 4)
    channel = r_send[0].astype(F32)
    for dy in GROUPS:
        dxs = [dx for dx in GROUPS if dx or dy]
        arrived(r_got.at[0 : len(dxs)], r_s, r_r.at[dy])
        for dx in dxs:
            channel = channel + r_got[dx * ny + dy].astype(F32)
    out_ref[...] = mixed_ref[...] + 0.5 * channel

    to_planes(lambda copy: copy.wait_send())
    to_sections(lambda copy: copy.wait_send())

    def gone(ref, sem):
        remote(ref, ref, sem, x_r.at[0], c=other).wait_send()

    gone(m_send.at[0 : ny - 1], ya_s.at[0])
    gone(gu_pack.at[0 : ny - 1], ya_s.at[1])
    gone(d_pack.at[0 : ny - 1], ya_s.at[2])
    gone(e_send.at[0 : ny - 1], e_s)
    gone(heads.at[0 : n_tp - 1], h_s)
    for way in range(2):
        gone(w_gu.at[0 : rounds[way]], ring_s.at[2 * way])
        gone(w_d.at[0 : rounds[way], pl.ds(0, UNITS)], ring_s.at[2 * way + 1])
    gone(r_got.at[0 : nx * ny - 1], a_s.at[0])
    gone(squares.at[0 : nx * ny - 1], a_s.at[1])
    gone(r_got.at[0 : nx * ny], p_s.at[0])
    gone(squares.at[0 : nx * ny], p_s.at[1])
    gone(w_d.at[0 : 2 * nx, pl.ds(0, UNITS)], d2_s)
    gone(hidden.at[0], x_s)
    gone(r_got.at[0 : nx * ny - 1], r_s)


def local(nz, ny, nx, *args):
    queries, keys, values, in_gate, forget_gate, stream = args[:6]
    head_gain, out_weight, norm_gain, gate_weight, up_weight, down_weight = args[6:]
    n_tp = 2 * nx
    dma = pltpu.SemaphoreType.DMA
    vmem = pltpu.VMEM
    slice_rows = T // ny
    shard = gate_weight.shape[0]
    scratch = [
        vmem((3, shard, T), F32),
        vmem((ny, shard, 3 * T), BF16),
        vmem((ny, shard, 2 * T), BF16),
        vmem((T, 2 * T), BF16),
        vmem((nz, T, 3 * T), BF16),
        vmem((nz, 256, T), BF16),
        vmem((nz // 2, 256, T), BF16),
        vmem((ny, slice_rows + 8, T), F32),
        vmem((ny, slice_rows + 8, T), F32),
        vmem((slice_rows + 8, T), BF16),
        vmem((SECTION, slice_rows + 8, T), BF16),
        vmem((slice_rows + 8, T), BF16),
        vmem((nz // SECTION, slice_rows + 8, T), BF16),
        vmem((ny, slice_rows + 8, T), F32),
        vmem((ny, slice_rows + 8, T), F32),
        vmem((n_tp, T, T), BF16),
        vmem((T, WIDE), F32),
        vmem((n_tp, ny * T, WIDE), BF16),
        vmem((n_tp * ny, 8, T), F32),
        vmem((2, ny * T, 2 * T), BF16),
        vmem((nx * ny, T, WIDE), BF16),
        vmem((nx * ny, T, WIDE), BF16),
        dma((3,)),
        dma((3,)),
        dma((SECTION,)),
        dma((SECTION,)),
        dma((nz - SECTION + 1,)),
        dma((nz // SECTION,)),
        dma,
        dma,
        dma((4,)),
        dma((2, 3, max(RING_ROUNDS) + 1)),
        dma,
        dma,
        dma((2,)),
        dma((2, ny)),
        dma((2,)),
        dma((2, ny)),
        dma,
        dma,
        dma,
        dma((ny,)),
        dma,
        dma((ny,)),
    ]
    return pl.pallas_call(
        functools.partial(kernel, nz, ny, nx),
        out_shape=jax.ShapeDtypeStruct((T, WIDE), F32),
        in_specs=[pl.BlockSpec(memory_space=vmem)] * 12,
        out_specs=pl.BlockSpec(memory_space=vmem),
        scratch_shapes=scratch,
        compiler_params=pltpu.CompilerParams(collective_id=0, has_side_effects=True),
        name="layer",
    )(
        queries,
        keys,
        values,
        in_gate,
        forget_gate,
        stream,
        head_gain.reshape(n_tp, T),
        out_weight,
        norm_gain.reshape(2 * n_tp, T),
        gate_weight,
        up_weight,
        down_weight,
    )


def solution(mesh):
    nz, ny, nx = 16, 4, mesh.shape["tp"] // 2
    finer = Mesh(mesh.devices.reshape(nz, ny, nx, 2), ("z", "y", "x", "c"))
    rows, columns = ("z", "y"), ("x", "c")
    in_specs = (
        P(rows, columns),
        P(rows, columns),
        P(rows, columns),
        P(columns, rows),
        P(columns, rows),
        P(rows, columns),
        P(),
        P(None, columns),
        P(),
        P(rows, columns),
        P(rows, columns),
        P(rows, columns),
    )
    return jax.shard_map(
        functools.partial(local, nz, ny, nx),
        mesh=finer,
        in_specs=in_specs,
        out_specs=P(rows, columns),
        check_vma=False,
    )
```

```python
import functools

import jax
import jax.numpy as jnp
from jax import lax
from jax.experimental import pallas as pl
from jax.experimental.pallas import tpu as pltpu
from jax.sharding import Mesh
from jax.sharding import PartitionSpec as P

MESH = pl.DeviceIdType.MESH
F32 = jnp.float32
BF16 = jnp.bfloat16

T = 128
WIDE = 256
UNITS = 176
EPS = 1e-6
FAR = -1e30
SECTION = 4
TURNS = ((0, 0), (6, 6), (3, 3), (5, 5), (4, 4))
FIRST = 3
GROUPS = (0, 3, 2, 1)
RING_ROUNDS = (8, 7)


def dot(a, b):
    return jnp.dot(a, b, preferred_element_type=F32)


def merge(early, late):
    memory_e, top_e, fall_e = early
    memory_l, top_l, fall_l = late
    top = jnp.maximum(fall_l + top_e, top_l)
    memory = jnp.exp(fall_l + top_e - top) * memory_e + jnp.exp(top_l - top) * memory_l
    return memory, top, fall_e + fall_l


def three_pieces(a):
    high = a.astype(BF16).astype(F32)
    rest = a - high
    middle = rest.astype(BF16).astype(F32)
    return high, middle, rest - middle


def kernel(
    nz,
    ny,
    nx,
    q_hbm,
    k_hbm,
    v_hbm,
    in_hbm,
    forget_hbm,
    stream_hbm,
    head_gain_hbm,
    out_w_hbm,
    norm_gain_hbm,
    gate_w_hbm,
    up_w_hbm,
    down_w_hbm,
    out_ref,
    q_ref,
    k_ref,
    v_ref,
    in_ref,
    forget_ref,
    stream_ref,
    head_gain_ref,
    out_w_ref,
    norm_gain_ref,
    gate_w_ref,
    up_w_ref,
    down_w_ref,
    load_s,
    tail,
    gu_pack,
    d_pack,
    d_block,
    w_gu,
    w_d,
    w_d2,
    m_send,
    m_got,
    z_send,
    z_got,
    s_send,
    s_got,
    e_send,
    e_got,
    heads,
    mixed_ref,
    acts,
    squares,
    hidden,
    ra_send,
    ra_got,
    rb_send,
    rb_got,
    sa_send,
    sa_got,
    sb_send,
    sb_got,
    entered,
    ya_s,
    ya_r,
    z_s,
    z_r,
    s_s,
    s_r,
    e_s,
    e_r,
    ring_s,
    ring_r,
    h_s,
    h_r,
    a_s,
    ax_r,
    ay_r,
    as_s,
    asx_r,
    asy_r,
    f_s,
    f_s2,
    fa_r,
    fb_r,
    p_s,
    p_r,
    ps_r,
    d2_s,
    d2_r,
    x_s,
    x_r,
    r_s,
    rb_s,
    ra_r,
    rb_r,
    s2_s,
    s3_s,
    sa_r,
    sb_r,
):
    z, y, x, c = (lax.axis_index(a) for a in ("z", "y", "x", "c"))
    tp = x * 2 + c
    n_tp = 2 * nx
    other = 1 - c

    def remote(src, dst, send, recv, **where):
        return pltpu.make_async_remote_copy(
            src_ref=src,
            dst_ref=dst,
            send_sem=send,
            recv_sem=recv,
            device_id=where,
            device_id_type=MESH,
        )

    def arrived(dst, send, recv):
        remote(dst, dst, send, recv, c=other).wait_recv()

    barrier = pltpu.get_barrier_semaphore()

    def greet(**where):
        pl.semaphore_signal(barrier, inc=1, device_id=where, device_id_type=MESH)

    for dz in range(1, nz):
        pl.when(z + dz < nz)(functools.partial(greet, z=z + dz))
    plane = [(dx, dy) for dx in range(nx) for dy in range(ny)]
    for dx, dy in plane:
        for dc in range(2):
            if dx or dy or dc:
                greet(x=lax.rem(x + dx, nx), y=lax.rem(y + dy, ny), c=lax.rem(c + dc, 2))

    pairs = (
        (in_hbm, in_ref),
        (forget_hbm, forget_ref),
        (k_hbm, k_ref),
        (v_hbm, v_ref),
        (gate_w_hbm, gate_w_ref),
        (up_w_hbm, up_w_ref),
        (down_w_hbm, down_w_ref),
        (q_hbm, q_ref),
        (stream_hbm, stream_ref),
        (head_gain_hbm, head_gain_ref),
        (norm_gain_hbm, norm_gain_ref),
        (out_w_hbm, out_w_ref),
    )
    loads = [
        pltpu.make_async_copy(hbm, ref, load_s.at[n]) for n, (hbm, ref) in enumerate(pairs)
    ]
    for copy in loads:
        copy.start()

    for copy in loads[0:4]:
        copy.wait()
    rows = lax.broadcasted_iota(jnp.int32, (T, T), 0)
    lanes = lax.broadcasted_iota(jnp.int32, (T, T), 1)
    causal = rows >= lanes
    same = rows == lanes
    forget = forget_ref[...]
    fall_each = jnp.minimum(forget, 0.0) - jnp.log1p(jnp.exp(-jnp.abs(forget)))
    in_row = in_ref[...]

    def column(row):
        return jnp.sum(jnp.where(same, jnp.broadcast_to(row, (T, T)), 0.0), axis=1, keepdims=True)

    fall_column = column(fall_each)
    in_column = column(in_row)
    cum_column = jnp.sum(
        jnp.where(causal, jnp.broadcast_to(fall_each, (T, T)), 0.0), axis=1, keepdims=True
    )
    cum_row = jnp.sum(
        jnp.where(rows <= lanes, jnp.broadcast_to(fall_column, (T, T)), 0.0), axis=0, keepdims=True
    )
    fall = jnp.broadcast_to(jnp.sum(fall_each, axis=1, keepdims=True), (1, T))
    log_weight = jnp.broadcast_to(fall - cum_column + in_column, (T, T))
    top = jnp.max(log_weight, axis=0, keepdims=True)
    weighted = jnp.exp(log_weight - top) * (T**-0.5) * k_ref[...].astype(F32)
    memory = lax.dot_general(
        weighted.astype(BF16), v_ref[...], (((0,), (0,)), ((), ())), preferred_element_type=F32
    )
    slice_rows = T // ny
    sub8 = lax.broadcasted_iota(jnp.int32, (8, T), 0)
    for j in range(ny):
        m_send[j, 0:slice_rows] = memory[j * slice_rows : (j + 1) * slice_rows]
        m_send[j, slice_rows : slice_rows + 8] = jnp.where(
            sub8 == 0, top, jnp.where(sub8 == 1, fall, 0.0)
        )
    m_got[y] = m_send[y]

    for copy in loads[4:7]:
        copy.wait()
    shard = gate_w_ref.shape[0]
    lane = lax.broadcasted_iota(jnp.int32, (shard, T), 1)
    ends = []
    for n, ref in enumerate((gate_w_ref, up_w_ref, down_w_ref)):
        tail[n] = jnp.zeros((shard, T), F32)
        tail[n, :, 0:64] = ref[:, 640:704].astype(F32)
        ends.append((ref[:, 512:640].astype(F32), tail[n]))

    def rest_of(n, j, at):
        wide, narrow = ends[n]
        wide = pltpu.roll(wide, (at - 32 * j) % T, 1)
        narrow = pltpu.roll(narrow, (at + 32 - 16 * j) % T, 1)
        here = (lane >= at) & (lane < at + 48)
        return jnp.where(here, jnp.where(lane < at + 32, wide, narrow), 0.0)

    for j in range(ny):
        gu_pack[j, :, 0:128] = gate_w_ref[:, j * T : (j + 1) * T]
        gu_pack[j, :, 128:256] = up_w_ref[:, j * T : (j + 1) * T]
        gu_pack[j, :, 256:384] = (rest_of(0, j, 0) + rest_of(1, j, 64)).astype(BF16)
        d_pack[j, :, 0:128] = down_w_ref[:, j * T : (j + 1) * T]
        d_pack[j, :, 128:256] = rest_of(2, j, 0).astype(BF16)

    def gu_rows(slot, begin, count):
        return w_gu.at[slot, pl.ds(pl.multiple_of(begin, 32), count), :]

    w_gu[z, pl.ds(pl.multiple_of(y * shard, 32), shard), :] = gu_pack[y]
    d_block[pl.ds(pl.multiple_of(y * shard, 32), shard), :] = d_pack[y]
    for s in range(nz):
        w_d[s, UNITS:256] = jnp.zeros((256 - UNITS, T), BF16)
    for s in range(nz // 2):
        w_d2[s, UNITS:256] = jnp.zeros((256 - UNITS, T), BF16)

    pl.semaphore_wait(barrier, 2 * nx * ny - 1 + z)
    section, place = z // SECTION, lax.rem(z, SECTION)
    for dz in range(1, nz):
        from_last = lax.rem(z + nz - dz, SECTION) == SECTION - 1
        awaited = from_last | (place >= dz) if dz < SECTION else from_last
        if dz == 1 or dz == nz - 1:
            awaited = True
        answer = functools.partial(
            pl.semaphore_signal, entered.at[dz], inc=1, device_id_type=MESH
        )
        pl.when((z >= dz) & awaited)(functools.partial(answer, device_id=dict(z=z - dz)))

    def is_in(dz):
        pl.semaphore_wait(entered.at[dz], 1)

    def send(*args, **where):
        remote(*args, **where).start()

    for dy in range(1, ny):
        to = lax.rem(y + dy, ny)
        send(m_send.at[to], m_got.at[y], ya_s.at[0], ya_r.at[0], y=to)
    for dy in range(1, ny):
        to = lax.rem(y + dy, ny)
        send(gu_pack.at[to], gu_rows(z, y * shard, shard), ya_s.at[1], ya_r.at[1], y=to)
        d_rows = pl.ds(pl.multiple_of(y * shard, 32), shard)
        send(d_pack.at[to], d_block.at[d_rows], ya_s.at[2], ya_r.at[2], y=to)

    for copy in loads[7:]:
        copy.wait()
    scores = lax.dot_general(
        q_ref[...], k_ref[...], (((1,), (1,)), ((), ())), preferred_element_type=F32
    ) * (T**-0.5)

    arrived(m_got.at[0 : ny - 1], ya_s.at[0], ya_r.at[0])
    state = (jnp.zeros((slice_rows, T), F32), jnp.full((1, T), FAR, F32), jnp.zeros((1, T), F32))
    before = []
    for j in range(ny):
        before.append(state)
        got = m_got[j]
        late = (
            got[0:slice_rows],
            got[slice_rows : slice_rows + 1],
            got[slice_rows + 1 : slice_rows + 2],
        )
        state = merge(state, late)
    plane_memory, plane_top, plane_fall = state

    def packed(memory, top, fall):
        numbers = jnp.zeros((8, T), F32)
        for n, piece in enumerate((*three_pieces(top), *three_pieces(fall))):
            numbers = jnp.where(sub8 == n, piece, numbers)
        return jnp.concatenate([memory, numbers], axis=0).astype(BF16)

    z_send[...] = packed(plane_memory, plane_top, plane_fall)

    def plane_part(dz):
        return remote(z_send, z_got.at[dz], z_s.at[dz], z_r.at[dz], z=z + dz)

    def section_part(dz):
        return remote(s_send, s_got.at[section], s_s.at[dz], s_r.at[section], z=z + dz)

    def to_planes(act):
        for dz in range(SECTION - 1, 0, -1):
            pl.when(place + dz < SECTION)(functools.partial(act, plane_part(dz)))

    def to_sections(act):
        for dz in range(nz - SECTION, 0, -1):
            due = (place == SECTION - 1) & (z + dz < nz)
            pl.when(due)(functools.partial(act, section_part(dz)))

    for dz in range(1, SECTION):
        pl.when(place + dz < SECTION)(functools.partial(is_in, dz))
    to_planes(lambda copy: copy.start())

    up_z, down_z = lax.rem(z + 1, nz), lax.rem(z + nz - 1, nz)
    rounds = RING_ROUNDS

    def ring_part(way, r, m, arriving):
        step = r if arriving else r - 1
        slot = lax.rem(z + step, nz) if way else lax.rem(z + nz - step, nz)
        ref = w_d.at[slot, pl.ds(0, UNITS)] if m == 2 else gu_rows(slot, m * (T // 2), T // 2)
        to = down_z if way else up_z
        return remote(ref, ref, ring_s.at[2 * way + m // 2], ring_r.at[way, m, r], z=to)

    def lend(slot):
        @pl.when(lax.rem(slot // 2, 2) == other)
        def _():
            there = w_d2.at[2 * (slot // 4) + lax.rem(slot, 2), pl.ds(0, UNITS)]
            send(w_d.at[slot, pl.ds(0, UNITS)], there, d2_s, d2_r, c=other)

    def ring_begin(way):
        for m in range(3):
            ring_part(way, 1, m, False).start()

    turns = [[(way, r, m) for r in range(1, rounds[way] + 1) for m in range(3)] for way in range(2)]

    def turn(way, r, m):
        ring_part(way, r, m, True).wait_recv()
        if r < rounds[way]:
            ring_part(way, r + 1, m, False).start()
        if m == 2:
            lend(lax.rem(z + r, nz) if way else lax.rem(z + nz - r, nz))

    def all_of(up, down):
        for n in range(max(len(up), len(down))):
            for n in [*up[n : n + 1], *down[n : n + 1]]:
                turn(*n)

    put_off = [[], []]

    def both_turns(stop):
        here = [turns[way][: TURNS[stop][way]] for way in range(2)]
        for way in range(2):
            del turns[way][: TURNS[stop][way]]
            put_off[way] += here[way]

        @pl.when(z >= FIRST)
        def _():
            all_of(*here)

    def put_off_turns(up, down):
        here = put_off[0][:up], put_off[1][:down]
        del put_off[0][:up], put_off[1][:down]

        @pl.when(z < FIRST)
        def _():
            all_of(*here)

    def rest_of_turns():
        @pl.when(z >= FIRST)
        def _():
            all_of(*turns)

        put_off_turns(*(len(p) for p in put_off))

        @pl.when(z < FIRST)
        def _():
            all_of(*turns)

    arrived(gu_pack.at[0 : ny - 1], ya_s.at[1], ya_r.at[1])
    arrived(d_pack.at[0 : ny - 1], ya_s.at[2], ya_r.at[2])
    turned = jnp.transpose(d_block[...].astype(F32))
    w_d[z, 0:UNITS] = turned[0:UNITS].astype(BF16)

    def passing(carry, got):
        total, highest, fallen = carry
        got = got.astype(F32)
        found = got[slice_rows : slice_rows + 8]
        level = found[0:1] + found[1:2] + found[2:3] + fallen
        new = jnp.maximum(highest, level)
        total = total * jnp.exp(highest - new) + jnp.exp(level - new) * got[0:slice_rows]
        return total, new, fallen + (found[3:4] + found[4:5] + found[5:6])

    def pass_plane(dz, carry):
        arrived(z_got.at[dz], z_s.at[dz], z_r.at[dz])
        return passing(carry, z_got[dz])

    def pass_section(n, carry):
        n = section - 1 - n
        arrived(s_got.at[n], s_s.at[0], s_r.at[n])
        return passing(carry, s_got[n])

    pl.when((place == SECTION - 1) & (z + 1 < nz))(functools.partial(is_in, 1))
    ring_begin(0)
    pl.when(z == 0)(functools.partial(is_in, nz - 1))
    ring_begin(1)
    lend(z)
    both_turns(0)
    passed = (jnp.zeros((slice_rows, T), F32), jnp.full((1, T), FAR, F32), jnp.zeros((1, T), F32))
    passed = lax.fori_loop(1, place + 1, pass_plane, passed)
    s_send[...] = packed(*merge(passed, (plane_memory, plane_top, plane_fall)))
    for dz in range(2, nz - SECTION + 1):
        due = (place == SECTION - 1) & (z + dz < nz)
        pl.when(due)(functools.partial(is_in, dz))
    to_sections(lambda copy: copy.start())
    both_turns(1)
    total, highest, fallen = lax.fori_loop(0, section, pass_section, passed)
    top_in = jnp.maximum(fallen, highest)
    plane_in = (total * jnp.exp(highest - top_in), top_in, jnp.zeros((1, T), F32))
    for j in range(ny):
        memory_j, top_j, _ = merge(plane_in, before[j])
        e_send[j, 0:slice_rows] = memory_j
        e_send[j, slice_rows : slice_rows + 8] = jnp.broadcast_to(top_j, (8, T))
    e_got[y] = e_send[y]
    for dy in range(1, ny):
        to = lax.rem(y + dy, ny)
        send(e_send.at[to], e_got.at[y], e_s, e_r, y=to)
    both_turns(2)
    arrived(e_got.at[0 : ny - 1], e_s, e_r)

    memory_in = jnp.concatenate([e_got[j, 0:slice_rows] for j in range(ny)], axis=0)
    top_here = e_got[0, slice_rows : slice_rows + 1]
    cum_wide = jnp.broadcast_to(cum_column, (T, T))
    carried = cum_wide + top_here
    spread = jnp.where(causal, cum_wide - cum_row + in_row, -jnp.inf)
    row_top = jnp.maximum(carried, jnp.max(spread, axis=1, keepdims=True))
    block_weights = (scores * jnp.exp(spread - row_top)).astype(BF16)
    inner = dot(block_weights, v_ref[...])
    outer = sum(dot(q_ref[...], piece.astype(BF16)) for piece in three_pieces(memory_in))
    readout = jnp.exp(carried - row_top) * outer + inner
    scale = lax.rsqrt(jnp.mean(readout * readout, axis=1, keepdims=True) + EPS)
    normed_heads = (readout * scale * head_gain_ref[pl.ds(tp, 1), :]).astype(BF16)
    heads[tp] = normed_heads
    for d in range(1, n_tp):
        to = lax.rem(tp + d, n_tp)
        send(heads.at[tp], heads.at[tp], h_s, h_r, x=to // 2, c=to % 2)

    both_turns(3)
    put_off_turns(4, 4)

    arrived(heads.at[0 : n_tp - 1], h_s, h_r)
    mixed = stream_ref[...].astype(F32)
    for n in range(nx):
        pair = jnp.concatenate([heads[2 * n], heads[2 * n + 1]], axis=1)
        mixed = mixed + dot(pair, out_w_ref[n * WIDE : (n + 1) * WIDE, :])
    mixed_ref[...] = mixed
    own_tokens = pl.ds(pl.multiple_of(y * T, T), T)
    for half in range(2):
        gain = norm_gain_ref[pl.ds(2 * tp + half, 1), :]
        part = mixed[:, half * T : (half + 1) * T]
        acts[tp, own_tokens, half * T : (half + 1) * T] = (part * gain).astype(BF16)
    square_column = jnp.sum(mixed * mixed, axis=1, keepdims=True)
    square_row = jnp.sum(
        jnp.where(same, jnp.broadcast_to(square_column, (T, T)), 0.0), axis=0, keepdims=True
    )
    squares[tp * ny + y] = jnp.broadcast_to(square_row, (8, T))

    def part_of(dx, dy, lanes, core):
        tokens = pl.ds(pl.multiple_of(lax.rem(y + ny - dy, ny) * T, T), T)
        return acts.at[lax.rem(x + nx - dx, nx) * 2 + core, tokens, lanes]

    def square_of(dx, dy):
        return squares.at[
            (lax.rem(x + nx - dx, nx) * 2 + c) * ny + lax.rem(y + ny - dy, ny)
        ]

    def to_partner(dx, dy, lanes, n, with_square=True):
        ref = part_of(dx, dy, lanes, c)
        send(ref, ref, p_s.at[0], p_r.at[n], c=other)
        if with_square:
            ref = square_of(dx, dy)
            send(ref, ref, p_s.at[1], ps_r.at[min(dy, 1)], c=other)

    ALL, LOW, HIGH = pl.ds(0, WIDE), pl.ds(0, T), pl.ds(T, T)
    own, own_square = part_of(0, 0, ALL, c), square_of(0, 0)
    for d in (2, 1, 3):
        there = dict(x=lax.rem(x + d, nx))
        send(own, own, a_s, ax_r.at[d], **there)
        send(own_square, own_square, as_s, asx_r, **there)
        there = dict(y=lax.rem(y + d, ny))
        send(own, own, a_s, ay_r.at[d], **there)
        send(own_square, own_square, as_s, asy_r, **there)
    to_partner(0, 0, ALL, 0)

    both_turns(4)
    put_off_turns(5, 5)
    arrived(squares.at[0:3], as_s, asx_r)
    for e in (1, 3, 2):
        arrived(ra_got.at[0:2], a_s, ax_r.at[e])
        for d in (2, 1, 3):
            there = dict(y=lax.rem(y + d, ny))
            ref = part_of(e, 0, LOW, c)
            send(ref, ref, f_s, fa_r, **there)
            ref = square_of(e, 0)
            send(ref, ref, as_s, asy_r, **there)
        arrived(ra_got.at[0:2], a_s, ay_r.at[e])
        for d in (2, 1, 3):
            ref = part_of(0, e, HIGH, c)
            send(ref, ref, f_s2, fb_r, x=lax.rem(x + d, nx))
        to_partner(e, 0, ALL, 0)
        to_partner(0, e, ALL, 1, False)
    def corners_on():
        corners = [(dx, dy) for dx in (1, 2, 3) for dy in (1, 2, 3)]
        arrived(ra_got.at[0:9], f_s, fa_r)
        for dx, dy in corners:
            to_partner(dx, dy, LOW, 2, False)
        arrived(squares.at[0:12], as_s, asy_r)
        for dx in range(nx):
            for dy in (1, 2, 3):
                ref = square_of(dx, dy)
                send(ref, ref, p_s.at[1], ps_r.at[1], c=other)
        arrived(ra_got.at[0:9], f_s, fb_r)
        for dx, dy in corners:
            to_partner(dx, dy, HIGH, 3, False)

    put_off_turns(7, 7)
    pl.when(z < FIRST)(corners_on)
    rest_of_turns()
    lane_wide = lax.broadcasted_iota(jnp.int32, (T, T), 1)

    def tokens_of(dy):
        return pl.ds(pl.multiple_of(lax.rem(y + ny - dy, ny) * T, T), T)

    def make_hidden(n):
        dy = GROUPS[n]
        tokens = tokens_of(dy)
        total_square = jnp.zeros((1, T), F32)
        both = jnp.zeros((T, 3 * T), F32)
        for b in range(n_tp):
            total_square = total_square + squares[b * ny + lax.rem(y + ny - dy, ny)][0:1]
            both = both + dot(acts[b, tokens, :], w_gu[2 * b : 2 * b + 2].reshape(2 * T, 3 * T))
        factor = lax.rsqrt(column(total_square) * (1.0 / (n_tp * WIDE)) + EPS)
        both = both * factor
        gate, up, rest = both[:, 0:T], both[:, T : 2 * T], both[:, 2 * T : 3 * T]
        here = slice(n * T, (n + 1) * T)
        hidden[c, here, 0:T] = (gate / (1.0 + jnp.exp(-gate)) * up).astype(BF16)
        small = rest / (1.0 + jnp.exp(-rest)) * pltpu.roll(rest, 64, 1)
        hidden[c, here, T : 2 * T] = jnp.where(lane_wide < 48, small, 0.0).astype(BF16)
        ref = hidden.at[c, here, :]
        send(ref, ref, x_s, x_r.at[n], c=other)

    arrived(ra_got.at[0 : 2 * nx], p_s.at[0], p_r.at[0])
    arrived(squares.at[0:nx], p_s.at[1], ps_r.at[0])
    make_hidden(0)
    pl.when(z >= FIRST)(corners_on)

    def share_out(first, last):
        for n in range(first, last):
            arrived(hidden.at[other, n * T : (n + 1) * T, :], x_s, x_r.at[n])
        mine, partners = (hidden[core, first * T : last * T, :] for core in (c, other))
        for dx in (2, 1, 3, 0):
            b = lax.rem(x + nx - dx, nx)
            own = jnp.concatenate([w_d[4 * b + 2 * c], w_d[4 * b + 2 * c + 1]], axis=1)
            theirs = jnp.concatenate([w_d2[2 * b], w_d2[2 * b + 1]], axis=1)
            share = (dot(mine, own) + dot(partners, theirs)).astype(BF16)
            for n in range(first, last):
                dy = GROUPS[n]
                at = slice((n - first) * T, (n - first + 1) * T)
                ra_send[dx * ny + dy] = share[at, 0:T]
                rb_send[dy * nx + dx] = share[at, T : 2 * T]
                if dx:
                    n_a = dx * ny + dy
                    send(ra_send.at[n_a], ra_got.at[n_a], r_s, ra_r.at[dy], x=b)
        for n in range(first, last):
            dy = GROUPS[n]
            if dy:
                block = pl.ds(dy * nx, nx)
                there = dict(y=lax.rem(y + ny - dy, ny))
                send(rb_send.at[block], rb_got.at[block], rb_s, rb_r, **there)

    arrived(ra_got.at[0:6], p_s.at[0], p_r.at[1])
    arrived(squares.at[0 : nx * (ny - 1)], p_s.at[1], ps_r.at[1])
    for n in (2, 3):
        arrived(ra_got.at[0:9], p_s.at[0], p_r.at[n])
    make_hidden(2)
    make_hidden(3)
    make_hidden(1)
    arrived(w_d2.at[0 : 2 * nx, pl.ds(0, UNITS)], d2_s, d2_r)
    share_out(2, 4)
    share_out(0, 2)

    def summed(first, got, places):
        total = first.astype(F32)
        for n in places:
            total = total + got[n].astype(F32)
        return total

    def low_sum(dy):
        arrived(ra_got.at[0 : nx - 1], r_s, ra_r.at[dy])
        return summed(ra_send[dy], ra_got, [dx * ny + dy for dx in range(1, nx)])

    for dy in (2, 1, 3):
        sa_send[dy] = low_sum(dy).astype(BF16)
        send(sa_send.at[dy], sa_got.at[dy], s2_s, sa_r, y=lax.rem(y + ny - dy, ny))
    arrived(rb_got.at[0 : nx * (ny - 1)], r_s, rb_r)

    def high_sum(dx):
        return summed(rb_send[dx], rb_got, [dy * nx + dx for dy in range(1, ny)])

    for dx in (2, 1, 3):
        sb_send[dx] = high_sum(dx).astype(BF16)
        send(sb_send.at[dx], sb_got.at[dx], s3_s, sb_r, x=lax.rem(x + nx - dx, nx))
    low, high = low_sum(0), high_sum(0)
    arrived(sa_got.at[0 : ny - 1], s2_s, sa_r)
    low = summed(low, sa_got, range(1, ny))
    out_ref[:, 0:T] = mixed_ref[:, 0:T] + 0.5 * low
    arrived(sb_got.at[0 : nx - 1], s2_s, sb_r)
    high = summed(high, sb_got, range(1, nx))
    out_ref[:, T:WIDE] = mixed_ref[:, T:WIDE] + 0.5 * high

    to_planes(lambda copy: copy.wait_send())
    to_sections(lambda copy: copy.wait_send())

    def gone(ref, sem):
        remote(ref, ref, sem, x_r.at[0], c=other).wait_send()

    gone(m_send.at[0 : ny - 1], ya_s.at[0])
    gone(gu_pack.at[0 : ny - 1], ya_s.at[1])
    gone(d_pack.at[0 : ny - 1], ya_s.at[2])
    gone(e_send.at[0 : ny - 1], e_s)
    gone(heads.at[0 : n_tp - 1], h_s)
    for way in range(2):
        gone(w_gu.at[0 : rounds[way]], ring_s.at[2 * way])
        gone(w_d.at[0 : rounds[way], pl.ds(0, UNITS)], ring_s.at[2 * way + 1])
    gone(ra_got.at[0:12], a_s)
    gone(squares.at[0:15], as_s)
    gone(ra_got.at[0:9], f_s)
    gone(rb_got.at[0:9], f_s2)
    gone(acts.at[0:nx], p_s.at[0])
    gone(squares.at[0 : nx * ny], p_s.at[1])
    gone(w_d.at[0 : 2 * nx, pl.ds(0, UNITS)], d2_s)
    gone(hidden.at[0], x_s)
    gone(ra_got.at[0 : nx * ny - ny], r_s)
    gone(rb_got.at[0 : nx * ny - nx], rb_s)
    gone(sa_got.at[0 : ny - 1], s2_s)
    gone(sb_got.at[0 : nx - 1], s3_s)


def local(nz, ny, nx, *args):
    queries, keys, values, in_gate, forget_gate, stream = args[:6]
    head_gain, out_weight, norm_gain, gate_weight, up_weight, down_weight = args[6:]
    n_tp = 2 * nx
    dma = pltpu.SemaphoreType.DMA
    vmem = pltpu.VMEM
    slice_rows = T // ny
    shard = gate_weight.shape[0]
    arrays = (
        queries,
        keys,
        values,
        in_gate,
        forget_gate,
        stream,
        head_gain.reshape(n_tp, T),
        out_weight,
        norm_gain.reshape(2 * n_tp, T),
        gate_weight,
        up_weight,
        down_weight,
    )
    scratch = [vmem(a.shape, a.dtype) for a in arrays]
    scratch += [
        dma((len(arrays),)),
        vmem((3, shard, T), F32),
        vmem((ny, shard, 3 * T), BF16),
        vmem((ny, shard, 2 * T), BF16),
        vmem((T, 2 * T), BF16),
        vmem((nz, T, 3 * T), BF16),
        vmem((nz, 256, T), BF16),
        vmem((nz // 2, 256, T), BF16),
        vmem((ny, slice_rows + 8, T), F32),
        vmem((ny, slice_rows + 8, T), F32),
        vmem((slice_rows + 8, T), BF16),
        vmem((SECTION, slice_rows + 8, T), BF16),
        vmem((slice_rows + 8, T), BF16),
        vmem((nz // SECTION, slice_rows + 8, T), BF16),
        vmem((ny, slice_rows + 8, T), F32),
        vmem((ny, slice_rows + 8, T), F32),
        vmem((n_tp, T, T), BF16),
        vmem((T, WIDE), F32),
        vmem((n_tp, ny * T, WIDE), BF16),
        vmem((n_tp * ny, 8, T), F32),
        vmem((2, ny * T, 2 * T), BF16),
        vmem((nx * ny, T, T), BF16),
        vmem((nx * ny, T, T), BF16),
        vmem((nx * ny, T, T), BF16),
        vmem((nx * ny, T, T), BF16),
        vmem((ny, T, T), BF16),
        vmem((ny, T, T), BF16),
        vmem((nx, T, T), BF16),
        vmem((nx, T, T), BF16),
        pltpu.SemaphoreType.REGULAR((nz,)),
        dma((3,)),
        dma((3,)),
        dma((SECTION,)),
        dma((SECTION,)),
        dma((nz - SECTION + 1,)),
        dma((nz // SECTION,)),
        dma,
        dma,
        dma((4,)),
        dma((2, 3, max(RING_ROUNDS) + 1)),
        dma,
        dma,
        dma,
        dma((nx,)),
        dma((ny,)),
        dma,
        dma,
        dma,
        dma,
        dma,
        dma,
        dma,
        dma((2,)),
        dma((4,)),
        dma((2,)),
        dma,
        dma,
        dma,
        dma((ny,)),
        dma,
        dma,
        dma((ny,)),
        dma,
        dma,
        dma,
        dma,
        dma,
    ]
    return pl.pallas_call(
        functools.partial(kernel, nz, ny, nx),
        out_shape=vmem((T, WIDE), F32),
        in_specs=[pl.BlockSpec(memory_space=pl.ANY)] * 12,
        out_specs=pl.BlockSpec(memory_space=vmem),
        scratch_shapes=scratch,
        compiler_params=pltpu.CompilerParams(collective_id=0, has_side_effects=True),
        name="layer",
    )(*arrays)


def solution(mesh):
    nz, ny, nx = 16, 4, mesh.shape["tp"] // 2
    finer = Mesh(mesh.devices.reshape(nz, ny, nx, 2), ("z", "y", "x", "c"))
    rows, columns = ("z", "y"), ("x", "c")
    in_specs = (
        P(rows, columns),
        P(rows, columns),
        P(rows, columns),
        P(columns, rows),
        P(columns, rows),
        P(rows, columns),
        P(),
        P(None, columns),
        P(),
        P(rows, columns),
        P(rows, columns),
        P(rows, columns),
    )
    return jax.shard_map(
        functools.partial(local, nz, ny, nx),
        mesh=finer,
        in_specs=in_specs,
        out_specs=P(rows, columns),
        check_vma=False,
    )
```

```python
import functools

import jax
import jax.numpy as jnp
from jax import lax
from jax.experimental import pallas as pl
from jax.experimental.pallas import tpu as pltpu
from jax.sharding import Mesh
from jax.sharding import PartitionSpec as P

MESH = pl.DeviceIdType.MESH
F32 = jnp.float32
BF16 = jnp.bfloat16

T = 128
WIDE = 256
UNITS = 176
EPS = 1e-6
FAR = -1e30
SECTION = 4
PIECES = ((0, 0, 32), (0, 32, 32), (0, 64, 32), (0, 96, 32), (1, 0, 96), (1, 96, 80))
TURNS = ((0, 0), (12, 13), (6, 6), (11, 11), (10, 10))
FIRST = 4
GROUPS = (0, 3, 2, 1)
RING_ROUNDS = (7, 8)


def dot(a, b):
    return jnp.dot(a, b, preferred_element_type=F32)


def merge(early, late):
    memory_e, top_e, fall_e = early
    memory_l, top_l, fall_l = late
    top = jnp.maximum(fall_l + top_e, top_l)
    memory = jnp.exp(fall_l + top_e - top) * memory_e + jnp.exp(top_l - top) * memory_l
    return memory, top, fall_e + fall_l


def three_pieces(a):
    high = a.astype(BF16).astype(F32)
    rest = a - high
    middle = rest.astype(BF16).astype(F32)
    return high, middle, rest - middle


def kernel(
    nz,
    ny,
    nx,
    q_hbm,
    k_hbm,
    v_hbm,
    in_hbm,
    forget_hbm,
    stream_hbm,
    head_gain_hbm,
    out_w_hbm,
    norm_gain_hbm,
    gate_w_hbm,
    up_w_hbm,
    down_w_hbm,
    out_ref,
    q_ref,
    k_ref,
    v_ref,
    in_ref,
    forget_ref,
    stream_ref,
    head_gain_ref,
    out_w_ref,
    norm_gain_ref,
    gate_w_ref,
    up_w_ref,
    down_w_ref,
    load_s,
    tail,
    gu_pack,
    d_pack,
    d_block,
    w_gu,
    w_d,
    w_d2,
    m_send,
    m_got,
    z_send,
    z_got,
    s_send,
    s_got,
    e_send,
    e_got,
    heads,
    mixed_ref,
    acts,
    squares,
    hidden,
    ra_send,
    ra_got,
    rb_send,
    rb_got,
    sa_send,
    sa_got,
    sb_send,
    sb_got,
    entered,
    ya_s,
    ya_r,
    z_s,
    z_r,
    s_s,
    s_r,
    e_s,
    e_r,
    ring_s,
    ring_r,
    h_s,
    h_r,
    a_s,
    ax_r,
    ay_r,
    as_s,
    asx_r,
    asy_r,
    f_s,
    f_s2,
    fa_r,
    fb_r,
    p_s,
    p_r,
    ps_r,
    d2_s,
    d2_r,
    x_s,
    x_r,
    r_s,
    rb_s,
    ra_r,
    rb_r,
    s2_s,
    s3_s,
    sa_r,
    sb_r,
):
    z, y, x, c = (lax.axis_index(a) for a in ("z", "y", "x", "c"))
    tp = x * 2 + c
    n_tp = 2 * nx
    other = 1 - c

    def remote(src, dst, send, recv, **where):
        return pltpu.make_async_remote_copy(
            src_ref=src,
            dst_ref=dst,
            send_sem=send,
            recv_sem=recv,
            device_id=where,
            device_id_type=MESH,
        )

    def arrived(dst, send, recv):
        remote(dst, dst, send, recv, c=other).wait_recv()

    barrier = pltpu.get_barrier_semaphore()

    def greet(**where):
        pl.semaphore_signal(barrier, inc=1, device_id=where, device_id_type=MESH)

    for dz in range(1, nz):
        pl.when(z + dz < nz)(functools.partial(greet, z=z + dz))
    plane = [(dx, dy) for dx in range(nx) for dy in range(ny)]
    for dx, dy in plane:
        for dc in range(2):
            if dx or dy or dc:
                greet(x=lax.rem(x + dx, nx), y=lax.rem(y + dy, ny), c=lax.rem(c + dc, 2))

    pairs = (
        (in_hbm, in_ref),
        (forget_hbm, forget_ref),
        (k_hbm, k_ref),
        (v_hbm, v_ref),
        (gate_w_hbm, gate_w_ref),
        (up_w_hbm, up_w_ref),
        (down_w_hbm, down_w_ref),
        (q_hbm, q_ref),
        (stream_hbm, stream_ref),
        (head_gain_hbm, head_gain_ref),
        (norm_gain_hbm, norm_gain_ref),
        (out_w_hbm, out_w_ref),
    )
    loads = [
        pltpu.make_async_copy(hbm, ref, load_s.at[n]) for n, (hbm, ref) in enumerate(pairs)
    ]
    for copy in loads:
        copy.start()

    for copy in loads[0:4]:
        copy.wait()
    rows = lax.broadcasted_iota(jnp.int32, (T, T), 0)
    lanes = lax.broadcasted_iota(jnp.int32, (T, T), 1)
    causal = rows >= lanes
    same = rows == lanes
    forget = forget_ref[...]
    fall_each = jnp.minimum(forget, 0.0) - jnp.log1p(jnp.exp(-jnp.abs(forget)))
    in_row = in_ref[...]

    def column(row):
        return jnp.sum(jnp.where(same, jnp.broadcast_to(row, (T, T)), 0.0), axis=1, keepdims=True)

    fall_column = column(fall_each)
    in_column = column(in_row)
    cum_column = jnp.sum(
        jnp.where(causal, jnp.broadcast_to(fall_each, (T, T)), 0.0), axis=1, keepdims=True
    )
    cum_row = jnp.sum(
        jnp.where(rows <= lanes, jnp.broadcast_to(fall_column, (T, T)), 0.0), axis=0, keepdims=True
    )
    fall = jnp.broadcast_to(jnp.sum(fall_each, axis=1, keepdims=True), (1, T))
    log_weight = jnp.broadcast_to(fall - cum_column + in_column, (T, T))
    top = jnp.max(log_weight, axis=0, keepdims=True)
    weighted = jnp.exp(log_weight - top) * (T**-0.5) * k_ref[...].astype(F32)
    memory = lax.dot_general(
        weighted.astype(BF16), v_ref[...], (((0,), (0,)), ((), ())), preferred_element_type=F32
    )
    slice_rows = T // ny
    sub8 = lax.broadcasted_iota(jnp.int32, (8, T), 0)
    for j in range(ny):
        m_send[j, 0:slice_rows] = memory[j * slice_rows : (j + 1) * slice_rows]
        m_send[j, slice_rows : slice_rows + 8] = jnp.where(
            sub8 == 0, top, jnp.where(sub8 == 1, fall, 0.0)
        )
    m_got[y] = m_send[y]

    for copy in loads[4:7]:
        copy.wait()
    shard = gate_w_ref.shape[0]
    lane = lax.broadcasted_iota(jnp.int32, (shard, T), 1)
    ends = []
    for n, ref in enumerate((gate_w_ref, up_w_ref, down_w_ref)):
        tail[n] = jnp.zeros((shard, T), F32)
        tail[n, :, 0:64] = ref[:, 640:704].astype(F32)
        ends.append((ref[:, 512:640].astype(F32), tail[n]))

    def rest_of(n, j, at):
        wide, narrow = ends[n]
        wide = pltpu.roll(wide, (at - 32 * j) % T, 1)
        narrow = pltpu.roll(narrow, (at + 32 - 16 * j) % T, 1)
        here = (lane >= at) & (lane < at + 48)
        return jnp.where(here, jnp.where(lane < at + 32, wide, narrow), 0.0)

    for j in range(ny):
        gu_pack[j, :, 0:128] = gate_w_ref[:, j * T : (j + 1) * T]
        gu_pack[j, :, 128:256] = up_w_ref[:, j * T : (j + 1) * T]
        gu_pack[j, :, 256:384] = (rest_of(0, j, 0) + rest_of(1, j, 64)).astype(BF16)
        d_pack[j, :, 0:128] = down_w_ref[:, j * T : (j + 1) * T]
        d_pack[j, :, 128:256] = rest_of(2, j, 0).astype(BF16)

    def gu_rows(slot, begin, count):
        return w_gu.at[slot, pl.ds(pl.multiple_of(begin, 32), count), :]

    w_gu[z, pl.ds(pl.multiple_of(y * shard, 32), shard), :] = gu_pack[y]
    d_block[pl.ds(pl.multiple_of(y * shard, 32), shard), :] = d_pack[y]
    for s in range(nz):
        w_d[s, UNITS:256] = jnp.zeros((256 - UNITS, T), BF16)
    for s in range(nz // 2):
        w_d2[s, UNITS:256] = jnp.zeros((256 - UNITS, T), BF16)

    pl.semaphore_wait(barrier, 2 * nx * ny - 1 + z)
    section, place = z // SECTION, lax.rem(z, SECTION)
    for dz in range(1, nz):
        from_last = lax.rem(z + nz - dz, SECTION) == SECTION - 1
        awaited = from_last | (place >= dz) if dz < SECTION else from_last
        if dz == 1 or dz == nz - 1:
            awaited = True
        answer = functools.partial(
            pl.semaphore_signal, entered.at[dz], inc=1, device_id_type=MESH
        )
        pl.when((z >= dz) & awaited)(functools.partial(answer, device_id=dict(z=z - dz)))

    def is_in(dz):
        pl.semaphore_wait(entered.at[dz], 1)

    def send(*args, **where):
        remote(*args, **where).start()

    for dy in range(1, ny):
        to = lax.rem(y + dy, ny)
        send(m_send.at[to], m_got.at[y], ya_s.at[0], ya_r.at[0], y=to)
    for dy in range(1, ny):
        to = lax.rem(y + dy, ny)
        send(gu_pack.at[to], gu_rows(z, y * shard, shard), ya_s.at[1], ya_r.at[1], y=to)
        d_rows = pl.ds(pl.multiple_of(y * shard, 32), shard)
        send(d_pack.at[to], d_block.at[d_rows], ya_s.at[2], ya_r.at[2], y=to)

    for copy in loads[7:]:
        copy.wait()
    scores = lax.dot_general(
        q_ref[...], k_ref[...], (((1,), (1,)), ((), ())), preferred_element_type=F32
    ) * (T**-0.5)

    arrived(m_got.at[0 : ny - 1], ya_s.at[0], ya_r.at[0])
    state = (jnp.zeros((slice_rows, T), F32), jnp.full((1, T), FAR, F32), jnp.zeros((1, T), F32))
    before = []
    for j in range(ny):
        before.append(state)
        got = m_got[j]
        late = (
            got[0:slice_rows],
            got[slice_rows : slice_rows + 1],
            got[slice_rows + 1 : slice_rows + 2],
        )
        state = merge(state, late)
    plane_memory, plane_top, plane_fall = state

    def packed(memory, top, fall):
        numbers = jnp.zeros((8, T), F32)
        for n, piece in enumerate((*three_pieces(top), *three_pieces(fall))):
            numbers = jnp.where(sub8 == n, piece, numbers)
        return jnp.concatenate([memory, numbers], axis=0).astype(BF16)

    z_send[...] = packed(plane_memory, plane_top, plane_fall)

    def plane_part(dz):
        return remote(z_send, z_got.at[dz], z_s.at[dz], z_r.at[dz], z=z + dz)

    def section_part(dz):
        return remote(s_send, s_got.at[section], s_s.at[dz], s_r.at[section], z=z + dz)

    def to_planes(act):
        for dz in range(SECTION - 1, 0, -1):
            pl.when(place + dz < SECTION)(functools.partial(act, plane_part(dz)))

    def to_sections(act):
        for dz in range(nz - SECTION, 0, -1):
            due = (place == SECTION - 1) & (z + dz < nz)
            pl.when(due)(functools.partial(act, section_part(dz)))

    for dz in range(1, SECTION):
        pl.when(place + dz < SECTION)(functools.partial(is_in, dz))
    to_planes(lambda copy: copy.start())

    up_z, down_z = lax.rem(z + 1, nz), lax.rem(z + nz - 1, nz)
    rounds = RING_ROUNDS

    def ring_part(way, r, m, arriving):
        step = r if arriving else r - 1
        slot = lax.rem(z + step, nz) if way else lax.rem(z + nz - step, nz)
        down, begin, count = PIECES[m]
        ref = w_d.at[slot, pl.ds(begin, count)] if down else gu_rows(slot, begin, count)
        to = down_z if way else up_z
        return remote(ref, ref, ring_s.at[2 * way + down], ring_r.at[way, m, r - 1], z=to)

    def lend(slot):
        @pl.when(lax.rem(slot // 2, 2) == other)
        def _():
            there = w_d2.at[2 * (slot // 4) + lax.rem(slot, 2), pl.ds(0, UNITS)]
            send(w_d.at[slot, pl.ds(0, UNITS)], there, d2_s, d2_r, c=other)

    def ring_begin(way):
        for m in range(len(PIECES)):
            ring_part(way, 1, m, False).start()

    turns = [[(way, r, m) for r in range(1, rounds[way] + 1) for m in range(len(PIECES))] for way in range(2)]

    def turn(way, r, m):
        ring_part(way, r, m, True).wait_recv()
        if r < rounds[way]:
            ring_part(way, r + 1, m, False).start()
        if m == len(PIECES) - 1:
            lend(lax.rem(z + r, nz) if way else lax.rem(z + nz - r, nz))

    def all_of(up, down):
        for n in range(max(len(up), len(down))):
            for n in [*up[n : n + 1], *down[n : n + 1]]:
                turn(*n)

    put_off = [[], []]

    def both_turns(stop):
        here = [turns[way][: TURNS[stop][way]] for way in range(2)]
        for way in range(2):
            del turns[way][: TURNS[stop][way]]
            put_off[way] += here[way]

        @pl.when(z >= FIRST)
        def _():
            all_of(*here)

    def put_off_turns(up, down):
        here = put_off[0][:up], put_off[1][:down]
        del put_off[0][:up], put_off[1][:down]

        @pl.when(z < FIRST)
        def _():
            all_of(*here)

    def rest_of_turns():
        @pl.when(z >= FIRST)
        def _():
            all_of(*turns)

        put_off_turns(*(len(p) for p in put_off))

        @pl.when(z < FIRST)
        def _():
            all_of(*turns)

    arrived(gu_pack.at[0 : ny - 1], ya_s.at[1], ya_r.at[1])
    arrived(d_pack.at[0 : ny - 1], ya_s.at[2], ya_r.at[2])
    turned = jnp.transpose(d_block[...].astype(F32))
    w_d[z, 0:UNITS] = turned[0:UNITS].astype(BF16)

    def passing(carry, got):
        total, highest, fallen = carry
        got = got.astype(F32)
        found = got[slice_rows : slice_rows + 8]
        level = found[0:1] + found[1:2] + found[2:3] + fallen
        new = jnp.maximum(highest, level)
        total = total * jnp.exp(highest - new) + jnp.exp(level - new) * got[0:slice_rows]
        return total, new, fallen + (found[3:4] + found[4:5] + found[5:6])

    def pass_plane(dz, carry):
        arrived(z_got.at[dz], z_s.at[dz], z_r.at[dz])
        return passing(carry, z_got[dz])

    def pass_section(n, carry):
        n = section - 1 - n
        arrived(s_got.at[n], s_s.at[0], s_r.at[n])
        return passing(carry, s_got[n])

    pl.when((place == SECTION - 1) & (z + 1 < nz))(functools.partial(is_in, 1))
    ring_begin(0)
    pl.when(z == 0)(functools.partial(is_in, nz - 1))
    ring_begin(1)
    lend(z)
    both_turns(0)
    passed = (jnp.zeros((slice_rows, T), F32), jnp.full((1, T), FAR, F32), jnp.zeros((1, T), F32))
    passed = lax.fori_loop(1, place + 1, pass_plane, passed)
    s_send[...] = packed(*merge(passed, (plane_memory, plane_top, plane_fall)))
    for dz in range(2, nz - SECTION + 1):
        due = (place == SECTION - 1) & (z + dz < nz)
        pl.when(due)(functools.partial(is_in, dz))
    to_sections(lambda copy: copy.start())
    both_turns(1)
    total, highest, fallen = lax.fori_loop(0, section, pass_section, passed)
    top_in = jnp.maximum(fallen, highest)
    plane_in = (total * jnp.exp(highest - top_in), top_in, jnp.zeros((1, T), F32))
    for j in range(ny):
        memory_j, top_j, _ = merge(plane_in, before[j])
        e_send[j, 0:slice_rows] = memory_j
        e_send[j, slice_rows : slice_rows + 8] = jnp.broadcast_to(top_j, (8, T))
    e_got[y] = e_send[y]
    for dy in range(1, ny):
        to = lax.rem(y + dy, ny)
        send(e_send.at[to], e_got.at[y], e_s, e_r, y=to)
    both_turns(2)
    arrived(e_got.at[0 : ny - 1], e_s, e_r)

    memory_in = jnp.concatenate([e_got[j, 0:slice_rows] for j in range(ny)], axis=0)
    top_here = e_got[0, slice_rows : slice_rows + 1]
    cum_wide = jnp.broadcast_to(cum_column, (T, T))
    carried = cum_wide + top_here
    spread = jnp.where(causal, cum_wide - cum_row + in_row, -jnp.inf)
    row_top = jnp.maximum(carried, jnp.max(spread, axis=1, keepdims=True))
    block_weights = (scores * jnp.exp(spread - row_top)).astype(BF16)
    inner = dot(block_weights, v_ref[...])
    outer = sum(dot(q_ref[...], piece.astype(BF16)) for piece in three_pieces(memory_in))
    readout = jnp.exp(carried - row_top) * outer + inner
    scale = lax.rsqrt(jnp.mean(readout * readout, axis=1, keepdims=True) + EPS)
    normed_heads = (readout * scale * head_gain_ref[pl.ds(tp, 1), :]).astype(BF16)
    heads[tp] = normed_heads
    for d in range(1, n_tp):
        to = lax.rem(tp + d, n_tp)
        send(heads.at[tp], heads.at[tp], h_s, h_r, x=to // 2, c=to % 2)

    both_turns(3)
    put_off_turns(8, 8)

    arrived(heads.at[0 : n_tp - 1], h_s, h_r)
    mixed = stream_ref[...].astype(F32)
    for n in range(nx):
        pair = jnp.concatenate([heads[2 * n], heads[2 * n + 1]], axis=1)
        mixed = mixed + dot(pair, out_w_ref[n * WIDE : (n + 1) * WIDE, :])
    mixed_ref[...] = mixed
    own_tokens = pl.ds(pl.multiple_of(y * T, T), T)
    for half in range(2):
        gain = norm_gain_ref[pl.ds(2 * tp + half, 1), :]
        part = mixed[:, half * T : (half + 1) * T]
        acts[tp, own_tokens, half * T : (half + 1) * T] = (part * gain).astype(BF16)
    square_column = jnp.sum(mixed * mixed, axis=1, keepdims=True)
    square_row = jnp.sum(
        jnp.where(same, jnp.broadcast_to(square_column, (T, T)), 0.0), axis=0, keepdims=True
    )
    squares[tp * ny + y] = jnp.broadcast_to(square_row, (8, T))

    def part_of(dx, dy, lanes, core):
        tokens = pl.ds(pl.multiple_of(lax.rem(y + ny - dy, ny) * T, T), T)
        return acts.at[lax.rem(x + nx - dx, nx) * 2 + core, tokens, lanes]

    def square_of(dx, dy):
        return squares.at[
            (lax.rem(x + nx - dx, nx) * 2 + c) * ny + lax.rem(y + ny - dy, ny)
        ]

    def to_partner(dx, dy, lanes, n, with_square=True):
        ref = part_of(dx, dy, lanes, c)
        send(ref, ref, p_s.at[0], p_r.at[n], c=other)
        if with_square:
            ref = square_of(dx, dy)
            send(ref, ref, p_s.at[1], ps_r.at[min(dy, 1)], c=other)

    ALL, LOW, HIGH = pl.ds(0, WIDE), pl.ds(0, T), pl.ds(T, T)
    own, own_square = part_of(0, 0, ALL, c), square_of(0, 0)
    for d in (2, 1, 3):
        there = dict(x=lax.rem(x + d, nx))
        send(own, own, a_s, ax_r.at[d], **there)
        send(own_square, own_square, as_s, asx_r, **there)
        there = dict(y=lax.rem(y + d, ny))
        send(own, own, a_s, ay_r.at[d], **there)
        send(own_square, own_square, as_s, asy_r, **there)
    to_partner(0, 0, ALL, 0)

    both_turns(4)
    put_off_turns(10, 10)
    arrived(squares.at[0:3], as_s, asx_r)
    for e in (1, 3, 2):
        arrived(ra_got.at[0:2], a_s, ax_r.at[e])
        for d in (2, 1, 3):
            there = dict(y=lax.rem(y + d, ny))
            ref = part_of(e, 0, LOW, c)
            send(ref, ref, f_s, fa_r.at[d], **there)
            ref = square_of(e, 0)
            send(ref, ref, as_s, asy_r, **there)
        arrived(ra_got.at[0:2], a_s, ay_r.at[e])
        for d in (2, 1, 3):
            ref = part_of(0, e, HIGH, c)
            send(ref, ref, f_s2, fb_r.at[d], x=lax.rem(x + d, nx))
        to_partner(e, 0, ALL, 0)
        to_partner(0, e, ALL, 1, False)
    def corners_on():
        for e in (1, 3, 2):
            arrived(ra_got.at[0:3], f_s, fa_r.at[e])
            for d in (1, 2, 3):
                to_partner(d, e, LOW, 2, False)
            arrived(ra_got.at[0:3], f_s, fb_r.at[e])
            for d in (1, 2, 3):
                to_partner(e, d, HIGH, 3, False)
        arrived(squares.at[0:12], as_s, asy_r)
        for dx in range(nx):
            for dy in (1, 2, 3):
                ref = square_of(dx, dy)
                send(ref, ref, p_s.at[1], ps_r.at[1], c=other)

    put_off_turns(14, 14)
    pl.when(z < FIRST)(corners_on)
    rest_of_turns()
    lane_wide = lax.broadcasted_iota(jnp.int32, (T, T), 1)

    def tokens_of(dy):
        return pl.ds(pl.multiple_of(lax.rem(y + ny - dy, ny) * T, T), T)

    def make_hidden(first, last):
        groups = range(first, last)
        both = jnp.zeros(((last - first) * T, 3 * T), F32)
        for b in range(n_tp):
            some = [acts[b, tokens_of(GROUPS[n]), :] for n in groups]
            some = jnp.concatenate(some, axis=0) if len(some) > 1 else some[0]
            both = both + dot(some, w_gu[2 * b : 2 * b + 2].reshape(2 * T, 3 * T))
        factors = []
        for n in groups:
            total_square = jnp.zeros((1, T), F32)
            for b in range(n_tp):
                there = b * ny + lax.rem(y + ny - GROUPS[n], ny)
                total_square = total_square + squares[there][0:1]
            factors.append(lax.rsqrt(column(total_square) * (1.0 / (n_tp * WIDE)) + EPS))
        for n in groups:
            part = both[(n - first) * T : (n - first + 1) * T] * factors[n - first]
            gate, up, rest = part[:, 0:T], part[:, T : 2 * T], part[:, 2 * T : 3 * T]
            here = slice(n * T, (n + 1) * T)
            hidden[c, here, 0:T] = (gate / (1.0 + jnp.exp(-gate)) * up).astype(BF16)
            small = rest / (1.0 + jnp.exp(-rest)) * pltpu.roll(rest, 64, 1)
            hidden[c, here, T : 2 * T] = jnp.where(lane_wide < 48, small, 0.0).astype(BF16)
            ref = hidden.at[c, here, :]
            send(ref, ref, x_s, x_r.at[n], c=other)

    arrived(ra_got.at[0 : 2 * nx], p_s.at[0], p_r.at[0])
    arrived(squares.at[0:nx], p_s.at[1], ps_r.at[0])
    make_hidden(0, 1)
    pl.when(z >= FIRST)(corners_on)

    def share_out(first, last):
        for n in range(first, last):
            arrived(hidden.at[other, n * T : (n + 1) * T, :], x_s, x_r.at[n])
        mine, partners = (hidden[core, first * T : last * T, :] for core in (c, other))
        def share_of(dx):
            b = lax.rem(x + nx - dx, nx)
            own = jnp.concatenate([w_d[4 * b + 2 * c], w_d[4 * b + 2 * c + 1]], axis=1)
            theirs = jnp.concatenate([w_d2[2 * b], w_d2[2 * b + 1]], axis=1)
            return (dot(mine, own) + dot(partners, theirs)).astype(BF16)

        def hand_out(dx, share):
            for n in range(first, last):
                dy = GROUPS[n]
                at = slice((n - first) * T, (n - first + 1) * T)
                n_a, n_b = dx * ny + dy, dy * nx + dx
                ra_send[n_a] = share[at, 0:T]
                rb_send[n_b] = share[at, T : 2 * T]
                if dx:
                    there = dict(x=lax.rem(x + nx - dx, nx))
                    send(ra_send.at[n_a], ra_got.at[n_a], r_s, ra_r.at[dy], **there)
                if dy:
                    there = dict(y=lax.rem(y + ny - dy, ny))
                    send(rb_send.at[n_b], rb_got.at[n_b], rb_s, rb_r, **there)

        ready = None
        for dx in (2, 1, 3, 0):
            share = share_of(dx)
            if ready is not None:
                hand_out(*ready)
            ready = dx, share
        hand_out(*ready)

    arrived(ra_got.at[0:6], p_s.at[0], p_r.at[1])
    arrived(squares.at[0 : nx * (ny - 1)], p_s.at[1], ps_r.at[1])
    for n in (2, 3):
        arrived(ra_got.at[0:9], p_s.at[0], p_r.at[n])
    make_hidden(1, 4)
    arrived(w_d2.at[0 : 2 * nx, pl.ds(0, UNITS)], d2_s, d2_r)
    share_out(2, 4)
    share_out(0, 2)

    def summed(first, got, places):
        total = first.astype(F32)
        for n in places:
            total = total + got[n].astype(F32)
        return total

    def low_sum(dy):
        arrived(ra_got.at[0 : nx - 1], r_s, ra_r.at[dy])
        return summed(ra_send[dy], ra_got, [dx * ny + dy for dx in range(1, nx)])

    for dy in (2, 1, 3):
        sa_send[dy] = low_sum(dy).astype(BF16)
        send(sa_send.at[dy], sa_got.at[dy], s2_s, sa_r, y=lax.rem(y + ny - dy, ny))
    arrived(rb_got.at[0 : nx * (ny - 1)], r_s, rb_r)

    def high_sum(dx):
        return summed(rb_send[dx], rb_got, [dy * nx + dx for dy in range(1, ny)])

    for dx in (2, 1, 3):
        sb_send[dx] = high_sum(dx).astype(BF16)
        send(sb_send.at[dx], sb_got.at[dx], s3_s, sb_r, x=lax.rem(x + nx - dx, nx))
    low, high = low_sum(0), high_sum(0)
    arrived(sa_got.at[0 : ny - 1], s2_s, sa_r)
    low = summed(low, sa_got, range(1, ny))
    out_ref[:, 0:T] = mixed_ref[:, 0:T] + 0.5 * low
    arrived(sb_got.at[0 : nx - 1], s2_s, sb_r)
    high = summed(high, sb_got, range(1, nx))
    out_ref[:, T:WIDE] = mixed_ref[:, T:WIDE] + 0.5 * high

    to_planes(lambda copy: copy.wait_send())
    to_sections(lambda copy: copy.wait_send())

    def gone(ref, sem):
        remote(ref, ref, sem, x_r.at[0], c=other).wait_send()

    gone(m_send.at[0 : ny - 1], ya_s.at[0])
    gone(gu_pack.at[0 : ny - 1], ya_s.at[1])
    gone(d_pack.at[0 : ny - 1], ya_s.at[2])
    gone(e_send.at[0 : ny - 1], e_s)
    gone(heads.at[0 : n_tp - 1], h_s)
    for way in range(2):
        gone(w_gu.at[0 : rounds[way]], ring_s.at[2 * way])
        gone(w_d.at[0 : rounds[way], pl.ds(0, UNITS)], ring_s.at[2 * way + 1])
    gone(ra_got.at[0:12], a_s)
    gone(squares.at[0:15], as_s)
    gone(ra_got.at[0:9], f_s)
    gone(rb_got.at[0:9], f_s2)
    gone(acts.at[0:nx], p_s.at[0])
    gone(squares.at[0 : nx * ny], p_s.at[1])
    gone(w_d.at[0 : 2 * nx, pl.ds(0, UNITS)], d2_s)
    gone(hidden.at[0], x_s)
    gone(ra_got.at[0 : nx * ny - ny], r_s)
    gone(rb_got.at[0 : nx * ny - nx], rb_s)
    gone(sa_got.at[0 : ny - 1], s2_s)
    gone(sb_got.at[0 : nx - 1], s3_s)


def local(nz, ny, nx, *args):
    queries, keys, values, in_gate, forget_gate, stream = args[:6]
    head_gain, out_weight, norm_gain, gate_weight, up_weight, down_weight = args[6:]
    n_tp = 2 * nx
    dma = pltpu.SemaphoreType.DMA
    vmem = pltpu.VMEM
    slice_rows = T // ny
    shard = gate_weight.shape[0]
    arrays = (
        queries,
        keys,
        values,
        in_gate,
        forget_gate,
        stream,
        head_gain.reshape(n_tp, T),
        out_weight,
        norm_gain.reshape(2 * n_tp, T),
        gate_weight,
        up_weight,
        down_weight,
    )
    scratch = [vmem(a.shape, a.dtype) for a in arrays]
    scratch += [
        dma((len(arrays),)),
        vmem((3, shard, T), F32),
        vmem((ny, shard, 3 * T), BF16),
        vmem((ny, shard, 2 * T), BF16),
        vmem((T, 2 * T), BF16),
        vmem((nz, T, 3 * T), BF16),
        vmem((nz, 256, T), BF16),
        vmem((nz // 2, 256, T), BF16),
        vmem((ny, slice_rows + 8, T), F32),
        vmem((ny, slice_rows + 8, T), F32),
        vmem((slice_rows + 8, T), BF16),
        vmem((SECTION, slice_rows + 8, T), BF16),
        vmem((slice_rows + 8, T), BF16),
        vmem((nz // SECTION, slice_rows + 8, T), BF16),
        vmem((ny, slice_rows + 8, T), F32),
        vmem((ny, slice_rows + 8, T), F32),
        vmem((n_tp, T, T), BF16),
        vmem((T, WIDE), F32),
        vmem((n_tp, ny * T, WIDE), BF16),
        vmem((n_tp * ny, 8, T), F32),
        vmem((2, ny * T, 2 * T), BF16),
        vmem((nx * ny, T, T), BF16),
        vmem((nx * ny, T, T), BF16),
        vmem((nx * ny, T, T), BF16),
        vmem((nx * ny, T, T), BF16),
        vmem((ny, T, T), BF16),
        vmem((ny, T, T), BF16),
        vmem((nx, T, T), BF16),
        vmem((nx, T, T), BF16),
        pltpu.SemaphoreType.REGULAR((nz,)),
        dma((3,)),
        dma((3,)),
        dma((SECTION,)),
        dma((SECTION,)),
        dma((nz - SECTION + 1,)),
        dma((nz // SECTION,)),
        dma,
        dma,
        dma((4,)),
        dma((2, len(PIECES), max(RING_ROUNDS))),
        dma,
        dma,
        dma,
        dma((nx,)),
        dma((ny,)),
        dma,
        dma,
        dma,
        dma,
        dma,
        dma((ny,)),
        dma((nx,)),
        dma((2,)),
        dma((4,)),
        dma((2,)),
        dma,
        dma,
        dma,
        dma((ny,)),
        dma,
        dma,
        dma((ny,)),
        dma,
        dma,
        dma,
        dma,
        dma,
    ]
    return pl.pallas_call(
        functools.partial(kernel, nz, ny, nx),
        out_shape=vmem((T, WIDE), F32),
        in_specs=[pl.BlockSpec(memory_space=pl.ANY)] * 12,
        out_specs=pl.BlockSpec(memory_space=vmem),
        scratch_shapes=scratch,
        compiler_params=pltpu.CompilerParams(collective_id=0, has_side_effects=True),
        name="layer",
    )(*arrays)


def solution(mesh):
    nz, ny, nx = 16, 4, mesh.shape["tp"] // 2
    finer = Mesh(mesh.devices.reshape(nz, ny, nx, 2), ("z", "y", "x", "c"))
    rows, columns = ("z", "y"), ("x", "c")
    in_specs = (
        P(rows, columns),
        P(rows, columns),
        P(rows, columns),
        P(columns, rows),
        P(columns, rows),
        P(rows, columns),
        P(),
        P(None, columns),
        P(),
        P(rows, columns),
        P(rows, columns),
        P(rows, columns),
    )
    return jax.shard_map(
        functools.partial(local, nz, ny, nx),
        mesh=finer,
        in_specs=in_specs,
        out_specs=P(rows, columns),
        check_vma=False,
    )
```
